256 devices in a mesh: sp: 16 (over y, x), dp: 16 (over z, core).
Axes of the slice: x: 4, y: 4, z: 8, core: 2. Of those that a mesh axis runs over, the one named last changes fastest.
Arguments:
- tokens: bfloat16 [16, 2048, 2048], P('dp', 'sp'), may hold values from -6 to 6
- query_weight: bfloat16 [2048, 1024], P('dp'), may hold values from -0.125 to 0.125
- key_weight: bfloat16 [2048, 1024], P('dp'), may hold values from -0.125 to 0.125
- value_weight: bfloat16 [2048, 2048], P('dp'), may hold values from -0.125 to 0.125
- output_weight: bfloat16 [2048, 2048], P('dp'), may hold values from -0.125 to 0.125
- log_decay: float32 [2, 16], P(None, 'sp'), may hold values from -0.04 to 0, as said below
Outputs:
- mixed: bfloat16 [16, 2048, 2048], P('dp', 'sp')
The draws below stay inside these ranges and needn't reach their ends.
Inputs may be any that keep to these rules, and one draw needn't show every extreme that they name: `log_decay`: every entry is negative: the logarithm of a head's decay per position.
All inputs are finite; a program needn't handle non-finite values.
Results may differ from the reference program's by a relative error of at most 0.012.
Values may be sent and summed in bfloat16 or wider, within the bound.
A program may use at most 128 MiB of HBM per device.

```python
import jax
import jax.numpy as jnp
from jax import lax

D = 2048
HEADS = 16
DK = 64
DV = 128
BLOCK = 512
SEQ = 2048
SEQS = 16


def draw_log_decay(key, part):
    first_key, second_key, third_key = jax.random.split(jax.random.fold_in(key, 17), 3)
    share = 0.5
    fast = jax.random.uniform(first_key, (2, HEADS), jnp.float32) < share
    fast_rate = jnp.exp(jax.random.uniform(second_key, (2, HEADS), jnp.float32, jnp.log(1.0 / 80.0), jnp.log(1.0 / 25.0)))
    slow_rate = jax.random.uniform(third_key, (2, HEADS), jnp.float32, 0.3, 2.0) / SEQ
    return (-jnp.where(fast, fast_rate, slow_rate)).astype(jnp.float32)


def level_of(rng, dims, shards, smallest, largest):
    factor_of, own = 1.0, jax.random.fold_in(rng, 6)
    for axis_at, shards_of in shards:
        draws = jnp.exp(jax.random.uniform(jax.random.fold_in(own, axis_at), (shards_of,), jnp.float32, smallest / len(shards), largest / len(shards)))
        factor_of = factor_of * jnp.repeat(draws, dims[axis_at] // shards_of).reshape([-1 if axis == axis_at else 1 for axis in range(len(dims))])
    return factor_of


def gaussian(key, extent, deviation, bound, cuts=(), kind=jnp.bfloat16):
    values = deviation * jax.random.normal(key, extent, jnp.float32)
    if cuts:
        values = values * level_of(key, extent, cuts, -0.22, 0.18)
    return jnp.clip(values, -bound, bound).astype(kind)


def setup_inputs(seed: int = 0) -> dict:
    splits = jax.random.split(jax.random.key(seed), 7)
    return {
        "tokens": gaussian(splits[0], (SEQS, SEQ, D), 1.0, 6.0, ((0, 16), (1, 16))),
        "query_weight": gaussian(splits[1], (D, HEADS * DK), D ** -0.5, 0.125, ((0, 16),)),
        "key_weight": gaussian(splits[2], (D, HEADS * DK), D ** -0.5, 0.125, ((0, 16),)),
        "value_weight": gaussian(splits[3], (D, HEADS * DV), D ** -0.5, 0.125, ((0, 16),)),
        "output_weight": gaussian(splits[4], (HEADS * DV, D), (HEADS * DV) ** -0.5, 0.125, ((0, 16),)),
        "log_decay": draw_log_decay(jax.random.fold_in(splits[6], 71), 0),
    }


exact_precision = lax.Precision.HIGHEST

def rotate(values_part, positions):
    half_dim = values_part.shape[-1] // 2
    frequency = 10000.0 ** (-jnp.arange(half_dim, dtype=jnp.float32) / half_dim)
    angles = positions[:, None] * frequency[None, :]
    cosine = jnp.cos(angles)[:, None, :]
    sine_part = jnp.sin(angles)[:, None, :]
    first = values_part[..., :half_dim]
    second = values_part[..., half_dim:]
    return jnp.concatenate([first * cosine - second * sine_part, first * sine_part + second * cosine], axis=-1)

def retain(query, key_rows, value_rows, log_rate):
    length, heads, key_dim = query.shape
    value_dim = value_rows.shape[-1]
    count = length // BLOCK
    offsets = jnp.arange(BLOCK, dtype=jnp.float32)
    distance = offsets[:, None] - offsets[None, :]
    decay_inner = jnp.where(distance[None] >= 0.0, jnp.exp(log_rate[:, None, None] * jnp.maximum(distance, 0.0)[None]), 0.0)
    decay_query = jnp.exp((offsets[:, None] + 1.0) * log_rate[None, :])[:, :, None]
    decay_key = jnp.exp((BLOCK - 1.0 - offsets)[:, None] * log_rate[None, :])[:, :, None]
    decay_block = jnp.exp(BLOCK * log_rate)[:, None, None]

    def blocks(array):
        return array.reshape(count, BLOCK, heads, array.shape[-1])

    def advance(state, inputs):
        query_block, key_block, value_block = inputs
        query_wide = query_block.astype(jnp.float32)
        key_wide = key_block.astype(jnp.float32)
        value_wide = value_block.astype(jnp.float32)
        inner = jnp.einsum('ihd,jhd->hij', query_wide, key_wide, precision=exact_precision) * decay_inner
        inner = inner.astype(jnp.bfloat16).astype(jnp.float32)
        result = jnp.einsum('hij,jhv->ihv', inner, value_wide, precision=exact_precision)
        result = result + jnp.einsum('ihd,hdv->ihv', query_wide * decay_query, state, precision=exact_precision)
        state = state * decay_block + jnp.einsum('jhd,jhv->hdv', key_wide * decay_key, value_wide, precision=exact_precision)
        return (state, result)
    initial = jnp.zeros((heads, key_dim, value_dim), jnp.float32)
    final_state, outputs = lax.scan(advance, initial, (blocks(query), blocks(key_rows), blocks(value_rows)))
    return outputs.reshape(length, heads, value_dim)

def mechanism(stacked, log_decay):
    length = stacked.shape[0]
    widened = stacked[..., :2 * DK].astype(jnp.float32)
    positions = jnp.arange(length, dtype=jnp.float32)
    query = rotate(widened[..., :DK], positions).astype(jnp.bfloat16)
    key_rows = rotate(widened[..., DK:2 * DK], positions).astype(jnp.bfloat16)
    value_rows = stacked[..., 2 * DK:]
    forward = retain(query, key_rows, value_rows, log_decay[0])
    backward = retain(jnp.flip(query, 0), jnp.flip(key_rows, 0), jnp.flip(value_rows, 0), log_decay[1])
    combined = forward + jnp.flip(backward, 0)
    average = lax.optimization_barrier(jnp.mean(combined, axis=-1, keepdims=True))
    centred = combined - average
    variance = lax.optimization_barrier(jnp.mean(centred * centred, axis=-1, keepdims=True))
    return (centred * lax.rsqrt(variance + 1e-06)).astype(jnp.bfloat16)

def reference(tokens, query_weight, key_weight, value_weight, output_weight, log_decay):

    def one_sequence(rows):
        length = rows.shape[0]
        query = jnp.dot(rows, query_weight, preferred_element_type=jnp.float32).astype(jnp.bfloat16).reshape(length, HEADS, DK)
        key_rows = jnp.dot(rows, key_weight, preferred_element_type=jnp.float32).astype(jnp.bfloat16).reshape(length, HEADS, DK)
        value_rows = jnp.dot(rows, value_weight, preferred_element_type=jnp.float32).astype(jnp.bfloat16).reshape(length, HEADS, DV)
        stacked = jnp.concatenate([query, key_rows, value_rows], axis=2)
        normed = mechanism(stacked, log_decay).reshape(length, HEADS * DV)
        return jnp.dot(normed, output_weight, preferred_element_type=jnp.float32).astype(jnp.bfloat16)
    return lax.map(one_sequence, tokens)
```

```python
import jax
import jax.numpy as jnp
import numpy as np
from jax import lax
from jax.experimental import pallas as pl
from jax.experimental.pallas import tpu as pltpu
from jax.sharding import PartitionSpec as P

D = 2048
HEADS = 16
DK = 64
DV = 128
BLOCK = 512
ROWS = 128
SIDE = 4
RING = 8
OWN = 4
PAIRS = 2
EPS = 1e-6

F32 = jnp.float32
BF16 = jnp.bfloat16


def mod(value, size):
    return lax.rem(value + size, size)


def matmul(a, b):
    return jnp.dot(a, b, preferred_element_type=F32)


def kernel(
    tok_hbm, q_hbm, k_hbm, v_hbm, o_hbm, ld_ref, freq_ref, out_ref,
    tok, wq, wo, rates, acc, cosine, sine, tiles, decay, qr, kr, vb, qs, ks,
    ab, states, carried, ret, ns, nb,
    local_sem, tok_s, tok_r, wq_s, wq_r, wqd_s, wqd_r, wo_s, wo_r,
    wy_s, wy_r, wf_s, wf_r, wod_s, wod_r, st_s, st_r, nb_s, nb_r, ld_s, ld_r,
):
    sp = lax.axis_index("sp")
    dp = lax.axis_index("dp")
    y, x = lax.div(sp, SIDE), lax.rem(sp, SIDE)
    z, c = lax.div(dp, 2), lax.rem(dp, 2)
    right, left, across = mod(x + 1, SIDE), mod(x - 1, SIDE), mod(x + 2, SIDE)
    above, below, facing = mod(y + 1, SIDE), mod(y - 1, SIDE), mod(y + 2, SIDE)

    def at_x(to):
        return (y * SIDE + to, dp)

    def at_y(to):
        return (to * SIDE + x, dp)

    def at_z(to):
        return (sp, to * 2 + c)

    other_core = (sp, z * 2 + (1 - c))
    sends = []

    def send(src, dst, send_sem, recv_sem, to):
        copy = pltpu.make_async_remote_copy(
            src_ref=src, dst_ref=dst, send_sem=send_sem, recv_sem=recv_sem,
            device_id=to, device_id_type=pl.DeviceIdType.MESH,
        )
        copy.start()
        sends.append(copy)

    def arrive(dst, send_sem, recv_sem):
        pltpu.make_async_remote_copy(
            src_ref=dst, dst_ref=dst, send_sem=send_sem, recv_sem=recv_sem,
            device_id=other_core, device_id_type=pl.DeviceIdType.MESH,
        ).wait_recv()

    locals_ = []

    def fetch(src, dst):
        copy = pltpu.make_async_copy(src, dst, local_sem.at[len(locals_)])
        copy.start()
        locals_.append(copy)

    fetch(tok_hbm.at[0], tok.at[x])
    fetch(q_hbm.at[:, pl.ds(pl.multiple_of(x * 256, 256), 256)], wq.at[dp, :, 0:256])
    fetch(k_hbm.at[:, pl.ds(pl.multiple_of(x * 256, 256), 256)], wq.at[dp, :, 256:512])
    fetch(v_hbm.at[:, pl.ds(pl.multiple_of(x * 512, 512), 512)], wq.at[dp, :, 512:1024])
    for part in range(SIDE):
        fetch(o_hbm.at[:, part * 512:(part + 1) * 512], wo.at[part, dp])

    barrier = pltpu.get_barrier_semaphore()
    peers = [(lax.rem(sp + o, SIDE * SIDE), dp) for o in range(1, SIDE * SIDE)]
    peers += [at_z(mod(z + 1, RING)), at_z(mod(z - 1, RING)), other_core]
    for peer in peers:
        pl.semaphore_signal(
            barrier, inc=1, device_id=peer, device_id_type=pl.DeviceIdType.MESH
        )
    pl.semaphore_wait(barrier, len(peers))

    def z_block(direction, step):
        return mod(z - step if direction == 0 else z + step, RING) * 2 + c

    def z_next(direction):
        return mod(z + 1 if direction == 0 else z - 1, RING)

    def half(direction):
        return pl.ds(0, 64) if direction == 0 else pl.ds(64, 64)

    def wq_part(direction, step):
        b = z_block(direction, step)
        return wq.at[b] if step < OWN else wq.at[b, half(direction)]

    def wo_part(direction, step):
        b = z_block(direction, step)
        return wo.at[y, b] if step < OWN else wo.at[y, b, half(direction)]

    def send_wq(step):
        for d in range(2):
            part = wq_part(d, step) if step < 3 else wq.at[z_block(d, step), half(d)]
            send(part, part, wq_s.at[d, step], wq_r.at[d, step], at_z(z_next(d)))

    def wait_wq(step):
        for d in range(2):
            arrive(wq_part(d, step), wq_s.at[d, step - 1], wq_r.at[d, step - 1])

    def send_wo(step):
        for d in range(2):
            part = wo_part(d, step) if step < 3 else wo.at[y, z_block(d, step), half(d)]
            send(part, part, wo_s.at[d, step], wo_r.at[d, step], at_z(z_next(d)))

    def wait_wo(step):
        for d in range(2):
            arrive(wo_part(d, step), wo_s.at[d, step - 1], wo_r.at[d, step - 1])

    def nth_block(n):
        if n == 0:
            return dp
        if n == 7:
            return z_block(0, 4)
        return z_block((n - 1) % 2, (n + 1) // 2)

    def swap_wq(n):
        b = nth_block(n)
        send(wq.at[b], wq.at[b], wqd_s.at[n], wqd_r.at[n], other_core)

    def take_wq(n):
        b = nth_block(n) + 1 - 2 * c
        arrive(wq.at[b], wqd_s.at[n], wqd_r.at[n])

    def swap_wo(n):
        b = nth_block(n)
        send(wo.at[:, b], wo.at[:, b], wod_s.at[n], wod_r.at[n], other_core)

    def take_wo(n):
        b = nth_block(n) + 1 - 2 * c
        arrive(wo.at[:, b], wod_s.at[n], wod_r.at[n])

    def spread_y(n):
        part = wo.at[y, nth_block(n)]
        send(part, part, wy_s.at[n, 0], wy_r.at[n, 0], at_y(above))
        send(part, part, wy_s.at[n, 1], wy_r.at[n, 1], at_y(below))

    def forward_y(n):
        b = nth_block(n)
        arrive(wo.at[below, b], wy_s.at[n, 0], wy_r.at[n, 0])
        arrive(wo.at[above, b], wy_s.at[n, 1], wy_r.at[n, 1])
        up, down = wo.at[below, b, half(0)], wo.at[above, b, half(1)]
        send(up, up, wf_s.at[n, 0], wf_r.at[n, 0], at_y(above))
        send(down, down, wf_s.at[n, 1], wf_r.at[n, 1], at_y(below))

    def finish_y(n):
        b = nth_block(n)
        arrive(wo.at[facing, b, half(0)], wf_s.at[n, 0], wf_r.at[n, 0])
        arrive(wo.at[facing, b, half(1)], wf_s.at[n, 1], wf_r.at[n, 1])
        swap_wo(n)

    locals_[0].wait()
    h0, h1 = pl.ds(0, 64), pl.ds(64, 64)
    send(tok.at[x, h0], tok.at[x, h0], tok_s.at[0], tok_r.at[0], at_x(right))
    send(tok.at[x, h1], tok.at[x, h1], tok_s.at[1], tok_r.at[1], at_x(left))
    send(tok.at[x, h1], tok.at[x, h1], tok_s.at[2], tok_r.at[2], at_x(right))
    send(tok.at[x, h0], tok.at[x, h0], tok_s.at[3], tok_r.at[3], at_x(left))
    for n in (1, 2, 3):
        locals_[n].wait()
    send_wq(0)
    for n in range(4, 8):
        locals_[n].wait()
    send_wo(0)
    swap_wq(0)
    for to in range(SIDE):
        @pl.when(jnp.logical_or(y != x, y != to))
        def _():
            copy = pltpu.make_async_remote_copy(
                src_ref=ld_ref, dst_ref=rates.at[x], send_sem=ld_s.at[to], recv_sem=ld_r.at[x],
                device_id=(to * SIDE + y, dp), device_id_type=pl.DeviceIdType.MESH,
            )
            copy.start()

        @pl.when(jnp.logical_and(y == x, y == to))
        def _():
            pltpu.make_async_copy(ld_ref, rates.at[x], ld_r.at[x]).start()

    swap_wo(0)

    lane = lax.broadcasted_iota(jnp.int32, (1, 128), 1)
    low = lax.rem(lane, 64) < 32
    for part in range(SIDE):
        rows = pl.ds(part * ROWS, ROWS)
        at = (lax.broadcasted_iota(jnp.int32, (ROWS, 128), 0) + (y * BLOCK + part * ROWS)).astype(F32)
        angle = at * freq_ref[...]
        cosine[rows, :] = jnp.cos(angle)
        turned = jnp.sin(angle)
        sine[rows, :] = jnp.where(low, -turned, turned)

    arrive(tok.at[left, h0], tok_s.at[0], tok_r.at[0])
    send(tok.at[left, h0], tok.at[left, h0], tok_s.at[4], tok_r.at[4], at_x(right))
    arrive(tok.at[right, h1], tok_s.at[1], tok_r.at[1])
    send(tok.at[right, h1], tok.at[right, h1], tok_s.at[5], tok_r.at[5], at_x(left))
    wait_wq(1)
    send_wq(1)
    swap_wq(1)
    swap_wq(2)

    for j in range(SIDE):
        arrive(rates.at[j], ld_s.at[j], ld_r.at[j])

    def decay_tiles(h, carry):
        a, b = rates[h, 0:1, :], rates[h, 1:2, :]
        i = lax.broadcasted_iota(jnp.int32, (ROWS, 128), 0)
        j = lax.broadcasted_iota(jnp.int32, (ROWS, 128), 1)
        for m in range(7):
            apart = (i - j + (3 - m) * ROWS).astype(F32)
            rate = jnp.where(apart >= 0.0, a, b)
            value = jnp.exp(rate * jnp.abs(apart))
            tiles[h, :, m * 128:(m + 1) * 128] = jnp.where(apart == 0.0, 2.0, value)
        return carry

    lax.fori_loop(0, OWN, decay_tiles, 0)

    first_head = lane < 64

    def decay_rows(p, carry):
        a = jnp.where(first_head, rates[2 * p, 0:1, :], rates[2 * p + 1, 0:1, :])
        b = jnp.where(first_head, rates[2 * p, 1:2, :], rates[2 * p + 1, 1:2, :])
        t = lax.broadcasted_iota(jnp.int32, (BLOCK, 128), 0).astype(F32)
        decay[p, 0] = jnp.exp((t + 1.0) * a)
        decay[p, 1] = jnp.exp((BLOCK - t) * b)
        decay[p, 2] = jnp.exp((BLOCK - 1.0 - t) * a)
        decay[p, 3] = jnp.exp(t * b)
        return carry

    lax.fori_loop(0, PAIRS, decay_rows, 0)

    wait_wo(1)
    send_wo(1)
    spread_y(1)
    spread_y(2)
    wait_wq(2)
    send_wq(2)
    swap_wq(3)
    swap_wq(4)
    forward_y(1)
    forward_y(2)
    wait_wo(2)
    send_wo(2)
    spread_y(3)
    spread_y(4)

    arrive(tok.at[left, h1], tok_s.at[2], tok_r.at[2])
    arrive(tok.at[right, h0], tok_s.at[3], tok_r.at[3])
    arrive(tok.at[across, h0], tok_s.at[4], tok_r.at[4])
    arrive(tok.at[across, h1], tok_s.at[5], tok_r.at[5])

    def project(at, fresh):
        rows = tok[:, :, pl.ds(pl.multiple_of(at * 256, 256), 256)].reshape(BLOCK, 256)
        for n in range(4):
            cols = slice(n * 256, (n + 1) * 256)
            weight = wq[pl.ds(at * 2, 2), :, cols].reshape(256, 256)
            part = matmul(rows, weight)
            acc[:, cols] = part if fresh else acc[:, cols] + part

    for n in range(5):
        take_wq(n)
    project(z, True)

    def project_offset(offset):
        project(mod(z + offset, RING), False)

    def project_many(first, count, stride):
        def step(i, carry):
            project_offset(first + i * stride)
            return carry
        lax.fori_loop(0, count, step, 0)

    project_many(1, 2, 1)
    project_many(6, 2, 1)
    wait_wq(3)
    send_wq(3)
    swap_wq(5)
    swap_wq(6)
    finish_y(1)
    finish_y(2)
    take_wq(5)
    take_wq(6)
    project_many(3, 2, 2)
    forward_y(3)
    forward_y(4)
    wait_wq(4)
    swap_wq(7)
    take_wq(7)
    project_offset(4)

    def turn(cols):
        flat = acc[:, cols].astype(BF16).astype(F32)
        partner = jnp.where(low, pltpu.roll(flat, 96, 1), pltpu.roll(flat, 32, 1))
        return (flat * cosine[...] + partner * sine[...]).astype(BF16)

    row_low = lax.broadcasted_iota(jnp.int32, (128, 1), 0) < 64
    for p in range(PAIRS):
        rq = turn(slice(p * 128, (p + 1) * 128))
        rk = turn(slice(256 + p * 128, 256 + (p + 1) * 128))
        qr[p] = rq
        kr[p] = rk
        value = acc[:, 512 + p * 256:512 + (p + 1) * 256].astype(BF16)
        vb[2 * p] = value[:, :128]
        vb[2 * p + 1] = value[:, 128:]
        wide_q, wide_k = rq.astype(F32), rk.astype(F32)
        qs[p, :, 0:128] = (wide_q * decay[p, 0]).astype(BF16)
        qs[p, :, 128:256] = (wide_q * decay[p, 1]).astype(BF16)
        ks[:, 0:128] = (wide_k * decay[p, 2]).astype(BF16)
        ks[:, 128:256] = (wide_k * decay[p, 3]).astype(BF16)
        both = lax.dot_general(
            ks[...], value, (((0,), (0,)), ((), ())), preferred_element_type=F32
        )
        for d in range(2):
            square = both[d * 128:(d + 1) * 128]
            ab[d, p] = jnp.where(row_low, square[:, :128], square[:, 128:]).astype(BF16)

    for n, to in enumerate((above, below, facing)):
        which = jnp.where(to > y, 0, 1)
        send(ab.at[which], states.at[y], st_s.at[n], st_r.at[n], at_y(to))

    wait_wo(3)
    send_wo(3)
    spread_y(5)
    spread_y(6)

    def in_block(r):
        rows = pl.ds(pl.multiple_of(r * ROWS, ROWS) if not isinstance(r, int) else r * ROWS, ROWS)
        cols = pl.ds(pl.multiple_of((3 - r) * 128, 128), BLOCK)
        for h in range(OWN):
            query = jnp.where((lane >= 64) == (h % 2 == 1), qr[h // 2, rows, :], jnp.zeros((), BF16))
            scores = lax.dot_general(
                query, kr[h // 2], (((1,), (1,)), ((), ())), preferred_element_type=F32
            )
            scores = (scores * tiles[h, :, cols]).astype(BF16)
            ret[r, :, h * 128:(h + 1) * 128] = matmul(scores, vb[h])

    in_block(0)
    in_block(1)
    finish_y(3)
    finish_y(4)
    wait_wo(4)
    spread_y(7)
    in_block(2)
    forward_y(5)
    forward_y(6)
    in_block(3)

    arrive(states.at[below], st_s.at[0], st_r.at[0])
    arrive(states.at[above], st_s.at[1], st_r.at[1])
    arrive(states.at[facing], st_s.at[2], st_r.at[2])
    for p in range(PAIRS):
        for d in range(2):
            rate = jnp.where(row_low, rates[2 * p, d:d + 1, 0:1], rates[2 * p + 1, d:d + 1, 0:1])
            total = jnp.zeros((128, 128), F32)
            for o in range(1, SIDE):
                source = mod(y - o if d == 0 else y + o, SIDE)
                there = (y - o >= 0) if d == 0 else (y + o < SIDE)
                weight = jnp.exp(rate * (BLOCK * (o - 1.0)))
                total = total + jnp.where(there, weight * states[source, p].astype(F32), 0.0)
            total = total.astype(BF16)
            zero = jnp.zeros((), BF16)
            carried[p, d * 128:(d + 1) * 128, 0:128] = jnp.where(row_low, total, zero)
            carried[p, d * 128:(d + 1) * 128, 128:256] = jnp.where(row_low, zero, total)

    def finish_rows(r, dst):
        for p in range(PAIRS):
            rows = pl.ds(pl.multiple_of(r * ROWS, ROWS) if not isinstance(r, int) else r * ROWS, ROWS)
            outside = matmul(qs[p, rows, :], carried[p])
            for e in range(2):
                h = 2 * p + e
                whole = ret[r, :, h * 128:(h + 1) * 128] + outside[:, e * 128:(e + 1) * 128]
                centred = whole - jnp.mean(whole, axis=-1, keepdims=True)
                var = jnp.mean(centred * centred, axis=-1, keepdims=True)
                dst[:, h * 128:(h + 1) * 128] = (centred * lax.rsqrt(var + EPS)).astype(BF16)

    for n, to in enumerate((across, left, right)):
        finish_rows(to, ns.at[n])
        send(ns.at[n], nb.at[x], nb_s.at[n], nb_r.at[n], at_x(to))
    finish_rows(x, nb.at[x])

    finish_y(5)
    finish_y(6)
    forward_y(7)
    finish_y(7)
    for n in range(8):
        take_wo(n)
    arrive(nb.at[across], nb_s.at[0], nb_r.at[0])
    arrive(nb.at[right], nb_s.at[1], nb_r.at[1])
    arrive(nb.at[left], nb_s.at[2], nb_r.at[2])

    for part in range(SIDE):
        total = jnp.zeros((ROWS, 512), F32)
        for g in range(SIDE):
            total = total + matmul(nb[g], wo[part, g * 4:(g + 1) * 4].reshape(512, 512))
        out_ref[0, :, part * 512:(part + 1) * 512] = total.astype(BF16)

    for copy in sends:
        copy.wait_send()
    for to in range(SIDE):
        @pl.when(jnp.logical_or(y != x, y != to))
        def _():
            pltpu.make_async_remote_copy(
                src_ref=ld_ref, dst_ref=rates.at[x], send_sem=ld_s.at[to], recv_sem=ld_r.at[x],
                device_id=(to * SIDE + y, dp), device_id_type=pl.DeviceIdType.MESH,
            ).wait_send()


def shards(tokens, query_weight, key_weight, value_weight, output_weight, log_decay):
    half_dim = DK // 2
    frequency = (
        np.float32(10000.0) ** (-np.arange(half_dim, dtype=np.float32) / np.float32(half_dim))
    ).astype(np.float32)
    frequency = jnp.asarray(np.tile(frequency, 4)[None, :])
    rate = jnp.broadcast_to(jnp.pad(log_decay, ((0, 6), (0, 0))), (8, 128))
    anywhere = pl.BlockSpec(memory_space=pl.ANY)
    vmem = pl.BlockSpec(memory_space=pltpu.VMEM)
    dma = pltpu.SemaphoreType.DMA
    return pl.pallas_call(
        kernel,
        out_shape=jax.ShapeDtypeStruct((1, ROWS, D), BF16),
        in_specs=[anywhere] * 5 + [vmem] * 2,
        out_specs=vmem,
        scratch_shapes=[
            pltpu.VMEM((SIDE, ROWS, D), BF16),
            pltpu.VMEM((16, 128, 1024), BF16),
            pltpu.VMEM((SIDE, 16, 128, 512), BF16),
            pltpu.VMEM((SIDE, 8, 128), F32),
            pltpu.VMEM((BLOCK, 1024), F32),
            pltpu.VMEM((BLOCK, 128), F32),
            pltpu.VMEM((BLOCK, 128), F32),
            pltpu.VMEM((OWN, ROWS, 7 * 128), F32),
            pltpu.VMEM((PAIRS, 4, BLOCK, 128), F32),
            pltpu.VMEM((PAIRS, BLOCK, 128), BF16),
            pltpu.VMEM((PAIRS, BLOCK, 128), BF16),
            pltpu.VMEM((OWN, BLOCK, 128), BF16),
            pltpu.VMEM((PAIRS, BLOCK, 256), BF16),
            pltpu.VMEM((BLOCK, 256), BF16),
            pltpu.VMEM((2, PAIRS, 128, 128), BF16),
            pltpu.VMEM((SIDE, PAIRS, 128, 128), BF16),
            pltpu.VMEM((PAIRS, 256, 256), BF16),
            pltpu.VMEM((SIDE, ROWS, 512), F32),
            pltpu.VMEM((3, ROWS, 512), BF16),
            pltpu.VMEM((SIDE, ROWS, 512), BF16),
            dma((8,)), dma((6,)), dma((6,)),
            dma((2, 4)), dma((2, 4)), dma((8,)), dma((8,)),
            dma((2, 4)), dma((2, 4)),
            dma((8, 2)), dma((8, 2)), dma((8, 2)), dma((8, 2)), dma((8,)), dma((8,)),
            dma((3,)), dma((3,)), dma((3,)), dma((3,)), dma((4,)), dma((4,)),
        ],
        compiler_params=pltpu.CompilerParams(
            collective_id=0, has_side_effects=True, vmem_limit_bytes=60 * 1024 * 1024
        ),
        name="retention",
    )(
        tokens, query_weight, key_weight, value_weight, output_weight, rate, frequency
    )


def solution(mesh):
    placed = (
        P("dp", "sp", None),
        P("dp", None),
        P("dp", None),
        P("dp", None),
        P("dp", None),
        P(None, "sp"),
    )
    return jax.shard_map(
        shards, mesh=mesh, in_specs=placed, out_specs=P("dp", "sp", None), check_vma=False
    )
```

```python
import jax
import jax.numpy as jnp
import numpy as np
from jax import lax
from jax.experimental import pallas as pl
from jax.experimental.pallas import tpu as pltpu
from jax.sharding import PartitionSpec as P

D = 2048
HEADS = 16
DK = 64
DV = 128
BLOCK = 512
ROWS = 128
SIDE = 4
RING = 8
OWN = 4
PAIRS = 2
EPS = 1e-6
KV = 768

F32 = jnp.float32
BF16 = jnp.bfloat16


def mod(value, size):
    return lax.rem(value + size, size)


def matmul(a, b):
    return jnp.dot(a, b, preferred_element_type=F32)


def kernel(
    tok_hbm, q_hbm, k_hbm, v_hbm, o_hbm, ld_ref, freq_ref, out_ref,
    tok, wq, wk, wo, own_rate, rates, acc_q, acc_k, cosine, sine, tiles, decay, qr, kr, vb, qs, ks,
    ab, states, carried, ret, ns, relay, nb, acc_o,
    local_sem, tok_s, tok_r, wq_s, wq_r, wqd_s, wqd_r, wk_s, wk_r, wkd_s, wkd_r, wo_s, wo_r,
    wy_s, wy_r, wf_s, wf_r, wod_s, wod_r, own_s, own_r, st_s, st_r, nb_s, nb_r, ld_s, ld_r,
):
    sp = lax.axis_index("sp")
    dp = lax.axis_index("dp")
    y, x = lax.div(sp, SIDE), lax.rem(sp, SIDE)
    z, c = lax.div(dp, 2), lax.rem(dp, 2)
    right, left, across = mod(x + 1, SIDE), mod(x - 1, SIDE), mod(x + 2, SIDE)
    above, below, facing = mod(y + 1, SIDE), mod(y - 1, SIDE), mod(y + 2, SIDE)
    h0, h1 = pl.ds(0, 64), pl.ds(64, 64)

    def at_x(to):
        return (y * SIDE + to, dp)

    def at_y(to):
        return (to * SIDE + x, dp)

    def at_z(to):
        return (sp, to * 2 + c)

    other_core = (sp, z * 2 + (1 - c))
    sends = []

    def send(src, dst, send_sem, recv_sem, to):
        copy = pltpu.make_async_remote_copy(
            src_ref=src, dst_ref=dst, send_sem=send_sem, recv_sem=recv_sem,
            device_id=to, device_id_type=pl.DeviceIdType.MESH,
        )
        copy.start()
        sends.append(copy)

    def arrive(dst, send_sem, recv_sem):
        pltpu.make_async_remote_copy(
            src_ref=dst, dst_ref=dst, send_sem=send_sem, recv_sem=recv_sem,
            device_id=other_core, device_id_type=pl.DeviceIdType.MESH,
        ).wait_recv()

    fetched = []

    def fetch(src, dst):
        copy = pltpu.make_async_copy(src, dst, local_sem.at[len(fetched)])
        copy.start()
        fetched.append(copy)

    for part in range(SIDE):
        fetch(o_hbm.at[:, part * 512:(part + 1) * 512], wo.at[part, dp])
    fetch(tok_hbm.at[0], tok.at[x])
    fetch(k_hbm.at[:, pl.ds(pl.multiple_of(x * 256, 256), 256)], wk.at[dp, :, 0:256])
    fetch(v_hbm.at[:, pl.ds(pl.multiple_of(x * 512, 512), 512)], wk.at[dp, :, 256:KV])
    fetch(q_hbm.at[:, pl.ds(pl.multiple_of(x * 256, 256), 256)], wq.at[dp])

    sub = lax.broadcasted_iota(jnp.int32, (8, 128), 0)
    own_rate[...] = jnp.where(sub == 0, ld_ref[0:1, 0:1], ld_ref[1:2, 0:1])

    barrier = pltpu.get_barrier_semaphore()
    peers = [(lax.rem(sp + o, SIDE * SIDE), dp) for o in range(1, SIDE * SIDE)]
    peers += [at_z(mod(z + 1, RING)), at_z(mod(z - 1, RING)), other_core]
    for peer in peers:
        pl.semaphore_signal(
            barrier, inc=1, device_id=peer, device_id_type=pl.DeviceIdType.MESH
        )
    pl.semaphore_wait(barrier, len(peers))
    for copy in fetched:
        copy.wait()

    def half(direction):
        return h0 if direction == 0 else h1

    def z_block(direction, step):
        return mod(z - step if direction == 0 else z + step, RING) * 2 + c

    def z_next(direction):
        return mod(z + 1 if direction == 0 else z - 1, RING)

    def nth_block(n):
        if n == 0:
            return dp
        if n == 7:
            return z_block(0, 4)
        return z_block((n - 1) % 2, (n + 1) // 2)

    def nth_other(n):
        return nth_block(n) + 1 - 2 * c

    def blocks_of(step):
        return (0,) if step == 0 else (2 * step - 1, 2 * step) if step < 4 else (7,)

    def ring_wait(view, step, s_sem, r_sem):
        if step > 0:
            for d in range(2):
                b = z_block(d, step)
                arrive(
                    view(b) if step < 4 else view(b, half(d)), s_sem.at[d, step - 1], r_sem.at[d, step - 1]
                )

    def ring_send(view, step, s_sem, r_sem):
        if step < 4:
            for d in range(2):
                b = z_block(d, step)
                part = view(b) if step < 3 else view(b, half(d))
                send(part, part, s_sem.at[d, step], r_sem.at[d, step], at_z(z_next(d)))

    def weight_step(ref, step, s_sem, r_sem, d_s, d_r):
        def view(b, rows=None):
            return ref.at[b] if rows is None else ref.at[b, rows]

        ring_wait(view, step, s_sem, r_sem)
        ring_send(view, step, s_sem, r_sem)
        for n in blocks_of(step):
            b = nth_block(n)
            send(ref.at[b], ref.at[b], d_s.at[n], d_r.at[n], other_core)

    def k_step(step):
        weight_step(wk, step, wk_s, wk_r, wkd_s, wkd_r)

    def q_step(step):
        weight_step(wq, step, wq_s, wq_r, wqd_s, wqd_r)

    def share(part, n, index):
        send(part, part, wod_s.at[n, index], wod_r.at[n, index], other_core)

    def o_step(step):
        def view(b, rows=None):
            return wo.at[y, b] if rows is None else wo.at[y, b, rows]

        ring_wait(view, step, wo_s, wo_r)
        ring_send(view, step, wo_s, wo_r)
        if step > 0:
            for n in blocks_of(step):
                part = wo.at[y, nth_block(n)]
                send(part, part, wy_s.at[n, 0], wy_r.at[n, 0], at_y(above))
                send(part, part, wy_s.at[n, 1], wy_r.at[n, 1], at_y(below))
                share(part, n, 0)

    def f_step(step):
        for n in blocks_of(step):
            b = nth_block(n)
            arrive(wo.at[below, b], wy_s.at[n, 0], wy_r.at[n, 0])
            arrive(wo.at[above, b], wy_s.at[n, 1], wy_r.at[n, 1])
            up, down = wo.at[below, b, h0], wo.at[above, b, h1]
            send(up, up, wf_s.at[n, 0], wf_r.at[n, 0], at_y(above))
            send(down, down, wf_s.at[n, 1], wf_r.at[n, 1], at_y(below))
            share(wo.at[below, b], n, 1)
            share(wo.at[above, b], n, 2)

    def g_step(step):
        for n in blocks_of(step):
            b = nth_block(n)
            arrive(wo.at[facing, b, h0], wf_s.at[n, 0], wf_r.at[n, 0])
            arrive(wo.at[facing, b, h1], wf_s.at[n, 1], wf_r.at[n, 1])
            share(wo.at[facing, b], n, 3)

    def own_output_block():
        send(wo.at[:, dp], wo.at[:, dp], own_s.at[0], own_r.at[0], other_core)

    def take_output(n):
        b = nth_other(n)
        if n == 0:
            arrive(wo.at[:, b], own_s.at[0], own_r.at[0])
        else:
            for index, part in enumerate((y, below, above, facing)):
                arrive(wo.at[part, b], wod_s.at[n, index], wod_r.at[n, index])

    def tokens_first():
        send(tok.at[x, h0], tok.at[x, h0], tok_s.at[0], tok_r.at[0], at_x(right))
        send(tok.at[x, h1], tok.at[x, h1], tok_s.at[1], tok_r.at[1], at_x(left))

    def tokens_second():
        send(tok.at[x, h1], tok.at[x, h1], tok_s.at[2], tok_r.at[2], at_x(right))
        send(tok.at[x, h0], tok.at[x, h0], tok_s.at[3], tok_r.at[3], at_x(left))

    def tokens_forward():
        arrive(tok.at[left, h0], tok_s.at[0], tok_r.at[0])
        send(tok.at[left, h0], tok.at[left, h0], tok_s.at[4], tok_r.at[4], at_x(right))
        arrive(tok.at[right, h1], tok_s.at[1], tok_r.at[1])
        send(tok.at[right, h1], tok.at[right, h1], tok_s.at[5], tok_r.at[5], at_x(left))

    def rate_copy(to):
        return pltpu.make_async_remote_copy(
            src_ref=own_rate, dst_ref=rates.at[x], send_sem=ld_s.at[to], recv_sem=ld_r.at[x],
            device_id=(to * SIDE + y, dp), device_id_type=pl.DeviceIdType.MESH,
        )

    def send_rates():
        for to in range(SIDE):
            @pl.when(jnp.logical_or(y != x, y != to))
            def _():
                rate_copy(to).start()

            @pl.when(jnp.logical_and(y == x, y == to))
            def _():
                pltpu.make_async_copy(own_rate, rates.at[x], ld_r.at[x]).start()

    lane = lax.broadcasted_iota(jnp.int32, (1, 128), 1)
    low = lax.rem(lane, 64) < 32

    def tables():
        for part in range(SIDE):
            rows = pl.ds(part * ROWS, ROWS)
            at = lax.broadcasted_iota(jnp.int32, (ROWS, 128), 0) + (y * BLOCK + part * ROWS)
            angle = at.astype(F32) * freq_ref[...]
            cosine[rows, :] = jnp.cos(angle)
            turned = jnp.sin(angle)
            sine[rows, :] = jnp.where(low, -turned, turned)

    def decays():
        for j in range(SIDE):
            arrive(rates.at[j], ld_s.at[j], ld_r.at[j])

        def decay_tiles(h, carry):
            a, b = rates[h, 0:1, :], rates[h, 1:2, :]
            i = lax.broadcasted_iota(jnp.int32, (ROWS, 128), 0)
            j = lax.broadcasted_iota(jnp.int32, (ROWS, 128), 1)
            for m in range(7):
                apart = (i - j + (3 - m) * ROWS).astype(F32)
                rate = jnp.where(apart >= 0.0, a, b)
                value = jnp.exp(rate * jnp.abs(apart))
                tiles[h, :, m * 128:(m + 1) * 128] = jnp.where(apart == 0.0, 2.0, value)
            return carry

        lax.fori_loop(0, OWN, decay_tiles, 0)
        first_head = lane < 64

        def decay_rows(p, carry):
            a = jnp.where(first_head, rates[2 * p, 0:1, :], rates[2 * p + 1, 0:1, :])
            b = jnp.where(first_head, rates[2 * p, 1:2, :], rates[2 * p + 1, 1:2, :])
            t = lax.broadcasted_iota(jnp.int32, (BLOCK, 128), 0).astype(F32)
            decay[p, 0] = jnp.exp((t + 1.0) * a)
            decay[p, 1] = jnp.exp((BLOCK - t) * b)
            decay[p, 2] = jnp.exp((BLOCK - 1.0 - t) * a)
            decay[p, 3] = jnp.exp(t * b)
            return carry

        lax.fori_loop(0, PAIRS, decay_rows, 0)

    def tokens_all():
        arrive(tok.at[left, h1], tok_s.at[2], tok_r.at[2])
        arrive(tok.at[right, h0], tok_s.at[3], tok_r.at[3])
        arrive(tok.at[across, h0], tok_s.at[4], tok_r.at[4])
        arrive(tok.at[across, h1], tok_s.at[5], tok_r.at[5])

    def project(ref, acc, width, offset, fresh):
        at = mod(z + offset, RING)
        rows = tok[:, :, pl.ds(pl.multiple_of(at * 256, 256), 256)].reshape(BLOCK, 256)
        for n in range(width // 256):
            cols = slice(n * 256, (n + 1) * 256)
            part = matmul(rows, ref[pl.ds(at * 2, 2), :, cols].reshape(256, 256))
            acc[:, cols] = part if fresh else acc[:, cols] + part

    def project_many(ref, acc, width, first, count, stride):
        def step(i, carry):
            project(ref, acc, width, first + i * stride, False)
            return carry

        lax.fori_loop(0, count, step, 0)

    def k_project(stage):
        k_or_q(stage, wk, acc_k, KV, wkd_s, wkd_r)

    def q_project(stage):
        k_or_q(stage, wq, acc_q, 256, wqd_s, wqd_r)

    def k_or_q(stage, ref, acc, width, d_s, d_r):
        for n in ((0, 1, 2), (3, 4), (5, 6), (7,))[stage]:
            arrive(ref.at[nth_other(n)], d_s.at[n], d_r.at[n])
        if stage == 0:
            project(ref, acc, width, 0, True)
            project_many(ref, acc, width, 1, 2, 6)
        elif stage == 3:
            project(ref, acc, width, 4, False)
        else:
            project_many(ref, acc, width, stage + 1, 2, 6 - 2 * stage)

    def turn(flat):
        wide = flat.astype(BF16).astype(F32)
        partner = jnp.where(low, pltpu.roll(wide, 96, 1), pltpu.roll(wide, 32, 1))
        return (wide * cosine[...] + partner * sine[...]).astype(BF16)

    row_low = lax.broadcasted_iota(jnp.int32, (128, 1), 0) < 64

    def keys_values():
        for p in range(PAIRS):
            rk = turn(acc_k[:, p * 128:(p + 1) * 128])
            kr[p] = rk
            value = acc_k[:, 256 + p * 256:256 + (p + 1) * 256].astype(BF16)
            vb[2 * p] = value[:, :128]
            vb[2 * p + 1] = value[:, 128:]
            wide_k = rk.astype(F32)
            ks[:, 0:128] = (wide_k * decay[p, 2]).astype(BF16)
            ks[:, 128:256] = (wide_k * decay[p, 3]).astype(BF16)
            both = lax.dot_general(
                ks[...], value, (((0,), (0,)), ((), ())), preferred_element_type=F32
            )
            for d in range(2):
                square = both[d * 128:(d + 1) * 128]
                ab[d, p] = jnp.where(row_low, square[:, :128], square[:, 128:]).astype(BF16)
        for n, to in ((2, facing), (0, above), (1, below)):
            send(ab.at[jnp.where(to > y, 0, 1)], states.at[y], st_s.at[n], st_r.at[n], at_y(to))

    def queries():
        for p in range(PAIRS):
            rq = turn(acc_q[:, p * 128:(p + 1) * 128])
            qr[p] = rq
            wide_q = rq.astype(F32)
            qs[p, :, 0:128] = (wide_q * decay[p, 0]).astype(BF16)
            qs[p, :, 128:256] = (wide_q * decay[p, 1]).astype(BF16)

    def in_block(r):
        rows = pl.ds(pl.multiple_of(r * ROWS, ROWS), ROWS)
        cols = pl.ds(pl.multiple_of((3 - r) * 128, 128), BLOCK)
        for h in range(OWN):
            query = jnp.where((lane >= 64) == (h % 2 == 1), qr[h // 2, rows, :], jnp.zeros((), BF16))
            scores = lax.dot_general(
                query, kr[h // 2], (((1,), (1,)), ((), ())), preferred_element_type=F32
            )
            scores = (scores * tiles[h, :, cols]).astype(BF16)
            ret[r, :, h * 128:(h + 1) * 128] = matmul(scores, vb[h])

    def carry_states():
        arrive(states.at[below], st_s.at[0], st_r.at[0])
        arrive(states.at[above], st_s.at[1], st_r.at[1])
        arrive(states.at[facing], st_s.at[2], st_r.at[2])
        for p in range(PAIRS):
            for d in range(2):
                rate = jnp.where(row_low, rates[2 * p, d:d + 1, 0:1], rates[2 * p + 1, d:d + 1, 0:1])
                total = jnp.zeros((128, 128), F32)
                for o in range(1, SIDE):
                    source = mod(y - o if d == 0 else y + o, SIDE)
                    there = (y - o >= 0) if d == 0 else (y + o < SIDE)
                    weight = jnp.exp(rate * (BLOCK * (o - 1.0)))
                    total = total + jnp.where(there, weight * states[source, p].astype(F32), 0.0)
                total = total.astype(BF16)
                zero = jnp.zeros((), BF16)
                carried[p, d * 128:(d + 1) * 128, 0:128] = jnp.where(row_low, total, zero)
                carried[p, d * 128:(d + 1) * 128, 128:256] = jnp.where(row_low, zero, total)

    def finish_rows(r, dst):
        rows = pl.ds(pl.multiple_of(r * ROWS, ROWS), ROWS)
        for p in range(PAIRS):
            outside = matmul(qs[p, rows, :], carried[p])
            for e in range(2):
                h = 2 * p + e
                whole = ret[r, :, h * 128:(h + 1) * 128] + outside[:, e * 128:(e + 1) * 128]
                centred = whole - jnp.mean(whole, axis=-1, keepdims=True)
                var = jnp.mean(centred * centred, axis=-1, keepdims=True)
                dst[:, h * 128:(h + 1) * 128] = (centred * lax.rsqrt(var + EPS)).astype(BF16)

    to_rows = (across, left, right, x)

    def normed(n):
        r = to_rows[n]
        if n == 3:
            finish_rows(r, nb.at[x])
            return
        finish_rows(r, ns.at[n])
        if n == 0:
            send(ns.at[0, h0], relay.at[0], nb_s.at[0], nb_r.at[0], at_x(right))
            send(ns.at[0, h1], relay.at[1], nb_s.at[1], nb_r.at[1], at_x(left))
        else:
            send(ns.at[n], nb.at[x], nb_s.at[n + 1], nb_r.at[n + 1], at_x(r))

    def normed_forward():
        arrive(relay.at[0], nb_s.at[0], nb_r.at[0])
        send(relay.at[0], nb.at[left, h0], nb_s.at[4], nb_r.at[4], at_x(right))
        arrive(relay.at[1], nb_s.at[1], nb_r.at[1])
        send(relay.at[1], nb.at[right, h1], nb_s.at[5], nb_r.at[5], at_x(left))

    def normed_all():
        arrive(nb.at[right], nb_s.at[2], nb_r.at[2])
        arrive(nb.at[left], nb_s.at[3], nb_r.at[3])
        arrive(nb.at[across, h0], nb_s.at[4], nb_r.at[4])
        arrive(nb.at[across, h1], nb_s.at[5], nb_r.at[5])

    def output(stage):
        if stage == 0:
            normed_all()
        for n in ((0, 1, 2, 3, 4), (5, 6, 7))[stage]:
            take_output(n)
        for part in range(SIDE):
            cols = slice(part * 512, (part + 1) * 512)
            total = jnp.zeros((ROWS, 512), F32) if stage == 0 else acc_o[:, cols]
            for offset in ((0, 1, 7, 2, 6), (3, 5, 4))[stage]:
                at = mod(z + offset, RING)
                lhs = nb[lax.div(at, 2), :, pl.ds(pl.multiple_of(lax.rem(at, 2) * 256, 256), 256)]
                total = total + matmul(lhs, wo[part, pl.ds(at * 2, 2)].reshape(256, 512))
            if stage == 0:
                acc_o[:, cols] = total
            else:
                out_ref[0, :, cols] = total.astype(BF16)

    def run(name, task, *arguments):
        with jax.named_scope(name):
            task(*arguments)

    run("O0", o_step, 0)
    run("K0", k_step, 0)
    run("T0", tokens_first)
    run("O1", o_step, 1)
    run("TAB", tables)
    run("Q0", q_step, 0)
    run("LD", send_rates)
    run("TF", tokens_forward)
    run("K1", k_step, 1)
    run("T1", tokens_second)
    run("SO0", own_output_block)
    run("DEC", decays)
    run("O2", o_step, 2)
    run("F1", f_step, 1)
    run("K2", k_step, 2)
    run("F2", f_step, 2)
    run("TA", tokens_all)
    run("KA", k_project, 0)
    run("Q1", q_step, 1)
    run("G1", g_step, 1)
    run("QA", q_project, 0)
    run("K3", k_step, 3)
    run("O3", o_step, 3)
    run("Q2", q_step, 2)
    run("KB", k_project, 1)
    run("KC", k_project, 2)
    run("K4", k_step, 4)
    run("KD", k_project, 3)
    run("RK", keys_values)
    run("Q3", q_step, 3)
    run("Q4", q_step, 4)
    run("G2", g_step, 2)
    run("QB", q_project, 1)
    run("QC", q_project, 2)
    run("O4", o_step, 4)
    run("F3", f_step, 3)
    run("QD", q_project, 3)
    run("RQ", queries)
    run("I0", in_block, to_rows[0])
    run("I1", in_block, to_rows[1])
    run("CAR", carry_states)
    run("N0", normed, 0)
    run("I2", in_block, to_rows[2])
    run("N1", normed, 1)
    run("N2", normed, 2)
    run("F4", f_step, 4)
    run("NF", normed_forward)
    run("G3", g_step, 3)
    run("I3", in_block, to_rows[3])
    run("G4", g_step, 4)
    run("N3", normed, 3)
    run("OA", output, 0)
    run("OB", output, 1)
    for copy in sends:
        copy.wait_send()
    for to in range(SIDE):
        @pl.when(jnp.logical_or(y != x, y != to))
        def _():
            rate_copy(to).wait_send()


def shards(tokens, query_weight, key_weight, value_weight, output_weight, log_decay):
    half_dim = DK // 2
    frequency = (
        np.float32(10000.0) ** (-np.arange(half_dim, dtype=np.float32) / np.float32(half_dim))
    ).astype(np.float32)
    frequency = jnp.asarray(np.tile(frequency, 4)[None, :])
    anywhere = pl.BlockSpec(memory_space=pl.ANY)
    vmem = pl.BlockSpec(memory_space=pltpu.VMEM)
    dma = pltpu.SemaphoreType.DMA
    return pl.pallas_call(
        kernel,
        out_shape=jax.ShapeDtypeStruct((1, ROWS, D), BF16),
        in_specs=[anywhere] * 5 + [vmem] * 2,
        out_specs=vmem,
        scratch_shapes=[
            pltpu.VMEM((SIDE, ROWS, D), BF16),
            pltpu.VMEM((16, 128, 256), BF16),
            pltpu.VMEM((16, 128, KV), BF16),
            pltpu.VMEM((SIDE, 16, 128, 512), BF16),
            pltpu.VMEM((8, 128), F32),
            pltpu.VMEM((SIDE, 8, 128), F32),
            pltpu.VMEM((BLOCK, 256), F32),
            pltpu.VMEM((BLOCK, KV), F32),
            pltpu.VMEM((BLOCK, 128), F32),
            pltpu.VMEM((BLOCK, 128), F32),
            pltpu.VMEM((OWN, ROWS, 7 * 128), F32),
            pltpu.VMEM((PAIRS, 4, BLOCK, 128), F32),
            pltpu.VMEM((PAIRS, BLOCK, 128), BF16),
            pltpu.VMEM((PAIRS, BLOCK, 128), BF16),
            pltpu.VMEM((OWN, BLOCK, 128), BF16),
            pltpu.VMEM((PAIRS, BLOCK, 256), BF16),
            pltpu.VMEM((BLOCK, 256), BF16),
            pltpu.VMEM((2, PAIRS, 128, 128), BF16),
            pltpu.VMEM((SIDE, PAIRS, 128, 128), BF16),
            pltpu.VMEM((PAIRS, 256, 256), BF16),
            pltpu.VMEM((SIDE, ROWS, 512), F32),
            pltpu.VMEM((3, ROWS, 512), BF16),
            pltpu.VMEM((2, 64, 512), BF16),
            pltpu.VMEM((SIDE, ROWS, 512), BF16),
            pltpu.VMEM((ROWS, D), F32),
            dma((8,)), dma((6,)), dma((6,)),
            dma((2, 4)), dma((2, 4)), dma((8,)), dma((8,)),
            dma((2, 4)), dma((2, 4)), dma((8,)), dma((8,)),
            dma((2, 4)), dma((2, 4)),
            dma((8, 2)), dma((8, 2)), dma((8, 2)), dma((8, 2)),
            dma((8, 4)), dma((8, 4)), dma((1,)), dma((1,)),
            dma((3,)), dma((3,)), dma((6,)), dma((6,)), dma((4,)), dma((4,)),
        ],
        compiler_params=pltpu.CompilerParams(
            collective_id=0, has_side_effects=True, vmem_limit_bytes=60 * 1024 * 1024
        ),
        name="retention",
    )(
        tokens, query_weight, key_weight, value_weight, output_weight, log_decay, frequency
    )


def solution(mesh):
    placed = (
        P("dp", "sp", None),
        P("dp", None),
        P("dp", None),
        P("dp", None),
        P("dp", None),
        P(None, "sp"),
    )
    return jax.shard_map(
        shards, mesh=mesh, in_specs=placed, out_specs=P("dp", "sp", None), check_vma=False
    )
```

```python
import jax
import jax.numpy as jnp
import numpy as np
from jax import lax
from jax.experimental import pallas as pl
from jax.experimental.pallas import tpu as pltpu
from jax.sharding import PartitionSpec as P

D = 2048
HEADS = 16
DK = 64
DV = 128
BLOCK = 512
ROWS = 128
SIDE = 4
RING = 8
OWN = 4
PAIRS = 2
EPS = 1e-6
KV = 768
PART = 384
REST = 512

F32 = jnp.float32
BF16 = jnp.bfloat16


def mod(value, size):
    return lax.rem(value + size, size)


def matmul(a, b):
    return jnp.dot(a, b, preferred_element_type=F32)


def kernel(
    tok_hbm, q_hbm, k_hbm, v_hbm, o_hbm, ld_ref, freq_ref, out_ref,
    tok, wq, wk, wo, wz, own_rate, rates, acc_q, acc_k, cosine, sine, tiles, decay, qr, kr, vb, qs, ks,
    ab, states, carried, ret, ns, relay, nb, acc_o,
    local_sem, tok_s, tok_r, wq_s, wq_r, wqd_s, wqd_r, wk_s, wk_r, wkd_s, wkd_r, wo_s, wo_r,
    wy_s, wy_r, wf_s, wf_r, wod_s, wod_r, own_s, own_r, wz_s, wz_r, wzd_s, wzd_r, st_s, st_r, nb_s, nb_r, ld_s, ld_r,
):
    sp = lax.axis_index("sp")
    dp = lax.axis_index("dp")
    y, x = lax.div(sp, SIDE), lax.rem(sp, SIDE)
    z, c = lax.div(dp, 2), lax.rem(dp, 2)
    right, left, across = mod(x + 1, SIDE), mod(x - 1, SIDE), mod(x + 2, SIDE)
    above, below, facing = mod(y + 1, SIDE), mod(y - 1, SIDE), mod(y + 2, SIDE)
    h0, h1 = pl.ds(0, 64), pl.ds(64, 64)

    def at_x(to):
        return (y * SIDE + to, dp)

    def at_y(to):
        return (to * SIDE + x, dp)

    def at_z(to):
        return (sp, to * 2 + c)

    other_core = (sp, z * 2 + (1 - c))
    sends = []

    def send(src, dst, send_sem, recv_sem, to):
        copy = pltpu.make_async_remote_copy(
            src_ref=src, dst_ref=dst, send_sem=send_sem, recv_sem=recv_sem,
            device_id=to, device_id_type=pl.DeviceIdType.MESH,
        )
        copy.start()
        sends.append(copy)

    def arrive(dst, send_sem, recv_sem):
        pltpu.make_async_remote_copy(
            src_ref=dst, dst_ref=dst, send_sem=send_sem, recv_sem=recv_sem,
            device_id=other_core, device_id_type=pl.DeviceIdType.MESH,
        ).wait_recv()

    fetched = []

    def fetch(src, dst):
        copy = pltpu.make_async_copy(src, dst, local_sem.at[len(fetched)])
        copy.start()
        fetched.append(copy)

    for part in range(SIDE):
        fetch(o_hbm.at[:, part * PART:(part + 1) * PART], wo.at[part, dp])
    fetch(o_hbm.at[:, SIDE * PART:D], wz.at[dp])
    fetch(tok_hbm.at[0], tok.at[x])
    fetch(k_hbm.at[:, pl.ds(pl.multiple_of(x * 256, 256), 256)], wk.at[dp, :, 0:256])
    fetch(v_hbm.at[:, pl.ds(pl.multiple_of(x * 512, 512), 512)], wk.at[dp, :, 256:KV])
    fetch(q_hbm.at[:, pl.ds(pl.multiple_of(x * 256, 256), 256)], wq.at[dp])

    sub = lax.broadcasted_iota(jnp.int32, (8, 128), 0)
    own_rate[...] = jnp.where(sub == 0, ld_ref[0:1, 0:1], ld_ref[0:1, 1:2])

    barrier = pltpu.get_barrier_semaphore()
    peers = [(lax.rem(sp + o, SIDE * SIDE), dp) for o in range(1, SIDE * SIDE)]
    peers += [at_z(mod(z + 1, RING)), at_z(mod(z - 1, RING)), other_core]
    for peer in peers:
        pl.semaphore_signal(
            barrier, inc=1, device_id=peer, device_id_type=pl.DeviceIdType.MESH
        )
    pl.semaphore_wait(barrier, len(peers))
    for copy in fetched:
        copy.wait()

    def half(direction):
        return h0 if direction == 0 else h1

    def z_block(direction, step):
        return mod(z - step if direction == 0 else z + step, RING) * 2 + c

    def z_next(direction):
        return mod(z + 1 if direction == 0 else z - 1, RING)

    def nth_block(n):
        if n == 0:
            return dp
        if n == 7:
            return z_block(0, 4)
        return z_block((n - 1) % 2, (n + 1) // 2)

    def nth_other(n):
        return nth_block(n) + 1 - 2 * c

    def blocks_of(step):
        return (0,) if step == 0 else (2 * step - 1, 2 * step) if step < 4 else (7,)

    def ring_wait(view, step, s_sem, r_sem):
        if step > 0:
            for d in range(2):
                b = z_block(d, step)
                arrive(
                    view(b) if step < 4 else view(b, half(d)), s_sem.at[d, step - 1], r_sem.at[d, step - 1]
                )

    def ring_send(view, step, s_sem, r_sem):
        if step < 4:
            for d in range(2):
                b = z_block(d, step)
                part = view(b) if step < 3 else view(b, half(d))
                send(part, part, s_sem.at[d, step], r_sem.at[d, step], at_z(z_next(d)))

    def weight_step(ref, step, s_sem, r_sem, d_s, d_r):
        def view(b, rows=None):
            return ref.at[b] if rows is None else ref.at[b, rows]

        ring_wait(view, step, s_sem, r_sem)
        ring_send(view, step, s_sem, r_sem)
        for n in blocks_of(step):
            b = nth_block(n)
            send(ref.at[b], ref.at[b], d_s.at[n], d_r.at[n], other_core)

    def k_step(step):
        weight_step(wk, step, wk_s, wk_r, wkd_s, wkd_r)

    def q_step(step):
        weight_step(wq, step, wq_s, wq_r, wqd_s, wqd_r)

    def zz_step(step):
        weight_step(wz, step, wz_s, wz_r, wzd_s, wzd_r)

    def share(part, n, index):
        send(part, part, wod_s.at[n, index], wod_r.at[n, index], other_core)

    def o_step(step):
        def view(b, rows=None):
            return wo.at[y, b] if rows is None else wo.at[y, b, rows]

        ring_wait(view, step, wo_s, wo_r)
        ring_send(view, step, wo_s, wo_r)
        if step > 0:
            for n in blocks_of(step):
                part = wo.at[y, nth_block(n)]
                send(part, part, wy_s.at[n, 0], wy_r.at[n, 0], at_y(above))
                send(part, part, wy_s.at[n, 1], wy_r.at[n, 1], at_y(below))
                share(part, n, 0)

    def f_step(step):
        for n in blocks_of(step):
            b = nth_block(n)
            arrive(wo.at[below, b], wy_s.at[n, 0], wy_r.at[n, 0])
            arrive(wo.at[above, b], wy_s.at[n, 1], wy_r.at[n, 1])
            up, down = wo.at[below, b, h0], wo.at[above, b, h1]
            send(up, up, wf_s.at[n, 0], wf_r.at[n, 0], at_y(above))
            send(down, down, wf_s.at[n, 1], wf_r.at[n, 1], at_y(below))
            share(wo.at[below, b], n, 1)
            share(wo.at[above, b], n, 2)

    def g_step(step):
        for n in blocks_of(step):
            b = nth_block(n)
            arrive(wo.at[facing, b, h0], wf_s.at[n, 0], wf_r.at[n, 0])
            arrive(wo.at[facing, b, h1], wf_s.at[n, 1], wf_r.at[n, 1])
            share(wo.at[facing, b], n, 3)

    def own_output_block():
        send(wo.at[:, dp], wo.at[:, dp], own_s.at[0], own_r.at[0], other_core)

    def take_output(n):
        b = nth_other(n)
        if n == 0:
            arrive(wo.at[:, b], own_s.at[0], own_r.at[0])
        else:
            for index, part in enumerate((y, below, above, facing)):
                arrive(wo.at[part, b], wod_s.at[n, index], wod_r.at[n, index])

    def tokens_first():
        send(tok.at[x, h0], tok.at[x, h0], tok_s.at[0], tok_r.at[0], at_x(right))
        send(tok.at[x, h1], tok.at[x, h1], tok_s.at[1], tok_r.at[1], at_x(left))

    def tokens_second():
        send(tok.at[x, h1], tok.at[x, h1], tok_s.at[2], tok_r.at[2], at_x(right))
        send(tok.at[x, h0], tok.at[x, h0], tok_s.at[3], tok_r.at[3], at_x(left))

    def tokens_forward():
        arrive(tok.at[left, h0], tok_s.at[0], tok_r.at[0])
        send(tok.at[left, h0], tok.at[left, h0], tok_s.at[4], tok_r.at[4], at_x(right))
        arrive(tok.at[right, h1], tok_s.at[1], tok_r.at[1])
        send(tok.at[right, h1], tok.at[right, h1], tok_s.at[5], tok_r.at[5], at_x(left))

    def rate_copy(to):
        return pltpu.make_async_remote_copy(
            src_ref=own_rate, dst_ref=rates.at[x], send_sem=ld_s.at[to], recv_sem=ld_r.at[x],
            device_id=(to * SIDE + y, dp), device_id_type=pl.DeviceIdType.MESH,
        )

    def send_rates():
        for to in range(SIDE):
            @pl.when(jnp.logical_or(y != x, y != to))
            def _():
                rate_copy(to).start()

            @pl.when(jnp.logical_and(y == x, y == to))
            def _():
                pltpu.make_async_copy(own_rate, rates.at[x], ld_r.at[x]).start()

    lane = lax.broadcasted_iota(jnp.int32, (1, 128), 1)
    low = lax.rem(lane, 64) < 32

    def tables():
        for part in range(SIDE):
            rows = pl.ds(part * ROWS, ROWS)
            at = lax.broadcasted_iota(jnp.int32, (ROWS, 128), 0) + (y * BLOCK + part * ROWS)
            angle = at.astype(F32) * freq_ref[...]
            cosine[rows, :] = jnp.cos(angle)
            turned = jnp.sin(angle)
            sine[rows, :] = jnp.where(low, -turned, turned)

    def decays():
        for j in range(SIDE):
            arrive(rates.at[j], ld_s.at[j], ld_r.at[j])

        def decay_tiles(h, carry):
            a, b = rates[h, 0:1, :], rates[h, 1:2, :]
            i = lax.broadcasted_iota(jnp.int32, (ROWS, 128), 0)
            j = lax.broadcasted_iota(jnp.int32, (ROWS, 128), 1)
            for m in range(7):
                apart = (i - j + (3 - m) * ROWS).astype(F32)
                rate = jnp.where(apart >= 0.0, a, b)
                value = jnp.exp(rate * jnp.abs(apart))
                tiles[h, :, m * 128:(m + 1) * 128] = jnp.where(apart == 0.0, 2.0, value)
            return carry

        lax.fori_loop(0, OWN, decay_tiles, 0)
        first_head = lane < 64

        def decay_rows(p, carry):
            a = jnp.where(first_head, rates[2 * p, 0:1, :], rates[2 * p + 1, 0:1, :])
            b = jnp.where(first_head, rates[2 * p, 1:2, :], rates[2 * p + 1, 1:2, :])
            t = lax.broadcasted_iota(jnp.int32, (BLOCK, 128), 0).astype(F32)
            decay[p, 0] = jnp.exp((t + 1.0) * a)
            decay[p, 1] = jnp.exp((BLOCK - t) * b)
            decay[p, 2] = jnp.exp((BLOCK - 1.0 - t) * a)
            decay[p, 3] = jnp.exp(t * b)
            return carry

        lax.fori_loop(0, PAIRS, decay_rows, 0)

    def tokens_all():
        arrive(tok.at[left, h1], tok_s.at[2], tok_r.at[2])
        arrive(tok.at[right, h0], tok_s.at[3], tok_r.at[3])
        arrive(tok.at[across, h0], tok_s.at[4], tok_r.at[4])
        arrive(tok.at[across, h1], tok_s.at[5], tok_r.at[5])

    def project(ref, acc, width, offset, fresh):
        at = mod(z + offset, RING)
        rows = tok[:, :, pl.ds(pl.multiple_of(at * 256, 256), 256)].reshape(BLOCK, 256)
        for n in range(width // 256):
            cols = slice(n * 256, (n + 1) * 256)
            part = matmul(rows, ref[pl.ds(at * 2, 2), :, cols].reshape(256, 256))
            acc[:, cols] = part if fresh else acc[:, cols] + part

    def project_many(ref, acc, width, first, count, stride):
        def step(i, carry):
            project(ref, acc, width, first + i * stride, False)
            return carry

        lax.fori_loop(0, count, step, 0)

    def k_project(stage):
        k_or_q(stage, wk, acc_k, KV, wkd_s, wkd_r)

    def q_project(stage):
        k_or_q(stage, wq, acc_q, 256, wqd_s, wqd_r)

    def k_or_q(stage, ref, acc, width, d_s, d_r):
        for n in ((0, 1, 2), (3, 4), (5, 6), (7,))[stage]:
            arrive(ref.at[nth_other(n)], d_s.at[n], d_r.at[n])
        if stage == 0:
            project(ref, acc, width, 0, True)
            project_many(ref, acc, width, 1, 2, 6)
        elif stage == 3:
            project(ref, acc, width, 4, False)
        else:
            project_many(ref, acc, width, stage + 1, 2, 6 - 2 * stage)

    def turn(flat):
        wide = flat.astype(BF16).astype(F32)
        partner = jnp.where(low, pltpu.roll(wide, 96, 1), pltpu.roll(wide, 32, 1))
        return (wide * cosine[...] + partner * sine[...]).astype(BF16)

    row_low = lax.broadcasted_iota(jnp.int32, (128, 1), 0) < 64

    def keys_values():
        for p in range(PAIRS):
            rk = turn(acc_k[:, p * 128:(p + 1) * 128])
            kr[p] = rk
            value = acc_k[:, 256 + p * 256:256 + (p + 1) * 256].astype(BF16)
            vb[2 * p] = value[:, :128]
            vb[2 * p + 1] = value[:, 128:]
            wide_k = rk.astype(F32)
            ks[:, 0:128] = (wide_k * decay[p, 2]).astype(BF16)
            ks[:, 128:256] = (wide_k * decay[p, 3]).astype(BF16)
            both = lax.dot_general(
                ks[...], value, (((0,), (0,)), ((), ())), preferred_element_type=F32
            )
            for d in range(2):
                square = both[d * 128:(d + 1) * 128]
                ab[d, p] = jnp.where(row_low, square[:, :128], square[:, 128:]).astype(BF16)
        for n, to in ((2, facing), (0, above), (1, below)):
            send(ab.at[jnp.where(to > y, 0, 1)], states.at[y], st_s.at[n], st_r.at[n], at_y(to))

    def queries():
        for p in range(PAIRS):
            rq = turn(acc_q[:, p * 128:(p + 1) * 128])
            qr[p] = rq
            wide_q = rq.astype(F32)
            qs[p, :, 0:128] = (wide_q * decay[p, 0]).astype(BF16)
            qs[p, :, 128:256] = (wide_q * decay[p, 1]).astype(BF16)

    def in_block(r):
        rows = pl.ds(pl.multiple_of(r * ROWS, ROWS), ROWS)
        cols = pl.ds(pl.multiple_of((3 - r) * 128, 128), BLOCK)
        for h in range(OWN):
            query = jnp.where((lane >= 64) == (h % 2 == 1), qr[h // 2, rows, :], jnp.zeros((), BF16))
            scores = lax.dot_general(
                query, kr[h // 2], (((1,), (1,)), ((), ())), preferred_element_type=F32
            )
            scores = (scores * tiles[h, :, cols]).astype(BF16)
            ret[r, :, h * 128:(h + 1) * 128] = matmul(scores, vb[h])

    def carry_states():
        arrive(states.at[below], st_s.at[0], st_r.at[0])
        arrive(states.at[above], st_s.at[1], st_r.at[1])
        arrive(states.at[facing], st_s.at[2], st_r.at[2])
        for p in range(PAIRS):
            for d in range(2):
                rate = jnp.where(row_low, rates[2 * p, d:d + 1, 0:1], rates[2 * p + 1, d:d + 1, 0:1])
                total = jnp.zeros((128, 128), F32)
                for o in range(1, SIDE):
                    source = mod(y - o if d == 0 else y + o, SIDE)
                    there = (y - o >= 0) if d == 0 else (y + o < SIDE)
                    weight = jnp.exp(rate * (BLOCK * (o - 1.0)))
                    total = total + jnp.where(there, weight * states[source, p].astype(F32), 0.0)
                total = total.astype(BF16)
                zero = jnp.zeros((), BF16)
                carried[p, d * 128:(d + 1) * 128, 0:128] = jnp.where(row_low, total, zero)
                carried[p, d * 128:(d + 1) * 128, 128:256] = jnp.where(row_low, zero, total)

    def finish_rows(r, dst):
        rows = pl.ds(pl.multiple_of(r * ROWS, ROWS), ROWS)
        for p in range(PAIRS):
            outside = matmul(qs[p, rows, :], carried[p])
            for e in range(2):
                h = 2 * p + e
                whole = ret[r, :, h * 128:(h + 1) * 128] + outside[:, e * 128:(e + 1) * 128]
                centred = whole - jnp.mean(whole, axis=-1, keepdims=True)
                var = jnp.mean(centred * centred, axis=-1, keepdims=True)
                dst[:, h * 128:(h + 1) * 128] = (centred * lax.rsqrt(var + EPS)).astype(BF16)

    to_rows = (across, left, right, x)

    def normed(n):
        r = to_rows[n]
        if n == 3:
            finish_rows(r, nb.at[x])
            return
        finish_rows(r, ns.at[n])
        if n == 0:
            send(ns.at[0, h0], relay.at[0], nb_s.at[0], nb_r.at[0], at_x(right))
            send(ns.at[0, h1], relay.at[1], nb_s.at[1], nb_r.at[1], at_x(left))
        else:
            send(ns.at[n], nb.at[x], nb_s.at[n + 1], nb_r.at[n + 1], at_x(r))

    def normed_forward():
        arrive(relay.at[0], nb_s.at[0], nb_r.at[0])
        send(relay.at[0], nb.at[left, h0], nb_s.at[4], nb_r.at[4], at_x(right))
        arrive(relay.at[1], nb_s.at[1], nb_r.at[1])
        send(relay.at[1], nb.at[right, h1], nb_s.at[5], nb_r.at[5], at_x(left))

    def normed_all():
        arrive(nb.at[right], nb_s.at[2], nb_r.at[2])
        arrive(nb.at[left], nb_s.at[3], nb_r.at[3])
        arrive(nb.at[across, h0], nb_s.at[4], nb_r.at[4])
        arrive(nb.at[across, h1], nb_s.at[5], nb_r.at[5])

    def output(stage):
        if stage == 0:
            normed_all()
        for n in ((0, 1, 2, 3, 4), (5, 6, 7))[stage]:
            take_output(n)
            arrive(wz.at[nth_other(n)], wzd_s.at[n], wzd_r.at[n])
        offsets = ((0, 1, 7, 2, 6), (3, 5, 4))[stage]
        left_hand, blocks = [], []
        for offset in offsets:
            at = mod(z + offset, RING)
            start = pl.multiple_of(lax.rem(at, 2) * 256, 256)
            left_hand.append(nb[lax.div(at, 2), :, pl.ds(start, 256)])
            blocks.append(pl.ds(at * 2, 2))
        for part in range(SIDE + 1):
            width = PART if part < SIDE else REST
            cols = slice(part * PART, part * PART + width)
            total = jnp.zeros((ROWS, width), F32) if stage == 0 else acc_o[:, cols]
            for lhs, rows in zip(left_hand, blocks):
                weight = wo[part, rows] if part < SIDE else wz[rows]
                total = total + matmul(lhs, weight.reshape(256, width))
            if stage == 0:
                acc_o[:, cols] = total
            else:
                out_ref[0, :, cols] = total.astype(BF16)

    def run(name, task, *arguments):
        with jax.named_scope(name):
            task(*arguments)

    run("K0", k_step, 0)
    run("Q0", q_step, 0)
    run("T0", tokens_first)
    run("LD", send_rates)
    run("T1", tokens_second)
    run("O0", o_step, 0)
    run("TAB", tables)
    run("K1", k_step, 1)
    run("O1", o_step, 1)
    run("TF", tokens_forward)
    run("Q1", q_step, 1)
    run("K2", k_step, 2)
    run("O2", o_step, 2)
    run("F1", f_step, 1)
    run("DEC", decays)
    run("TA", tokens_all)
    run("KA", k_project, 0)
    run("KB", k_project, 1)
    run("K3", k_step, 3)
    run("F2", f_step, 2)
    run("Q2", q_step, 2)
    run("Z0", zz_step, 0)
    run("O3", o_step, 3)
    run("KC", k_project, 2)
    run("K4", k_step, 4)
    run("KD", k_project, 3)
    run("G2", g_step, 2)
    run("RK", keys_values)
    run("Q3", q_step, 3)
    run("QA", q_project, 0)
    run("QB", q_project, 1)
    run("Z1", zz_step, 1)
    run("G1", g_step, 1)
    run("QC", q_project, 2)
    run("Q4", q_step, 4)
    run("O4", o_step, 4)
    run("SO0", own_output_block)
    run("QD", q_project, 3)
    run("RQ", queries)
    run("I1", in_block, to_rows[1])
    run("I0", in_block, to_rows[0])
    run("Z2", zz_step, 2)
    run("CAR", carry_states)
    run("N0", normed, 0)
    run("N1", normed, 1)
    run("I2", in_block, to_rows[2])
    run("N2", normed, 2)
    run("F3", f_step, 3)
    run("I3", in_block, to_rows[3])
    run("F4", f_step, 4)
    run("N3", normed, 3)
    run("NF", normed_forward)
    run("Z3", zz_step, 3)
    run("G3", g_step, 3)
    run("G4", g_step, 4)
    run("Z4", zz_step, 4)
    run("OA", output, 0)
    run("OB", output, 1)
    for copy in sends:
        copy.wait_send()
    for to in range(SIDE):
        @pl.when(jnp.logical_or(y != x, y != to))
        def _():
            rate_copy(to).wait_send()


def shards(tokens, query_weight, key_weight, value_weight, output_weight, log_decay):
    half_dim = DK // 2
    frequency = (
        np.float32(10000.0) ** (-np.arange(half_dim, dtype=np.float32) / np.float32(half_dim))
    ).astype(np.float32)
    frequency = jnp.asarray(np.tile(frequency, 4)[None, :])
    anywhere = pl.BlockSpec(memory_space=pl.ANY)
    vmem = pl.BlockSpec(memory_space=pltpu.VMEM)
    dma = pltpu.SemaphoreType.DMA
    return pl.pallas_call(
        kernel,
        out_shape=pltpu.VMEM((1, ROWS, D), BF16),
        in_specs=[anywhere] * 5 + [vmem] * 2,
        out_specs=vmem,
        scratch_shapes=[
            pltpu.VMEM((SIDE, ROWS, D), BF16),
            pltpu.VMEM((16, 128, 256), BF16),
            pltpu.VMEM((16, 128, KV), BF16),
            pltpu.VMEM((SIDE, 16, 128, PART), BF16),
            pltpu.VMEM((16, 128, REST), BF16),
            pltpu.VMEM((8, 128), F32),
            pltpu.VMEM((SIDE, 8, 128), F32),
            pltpu.VMEM((BLOCK, 256), F32),
            pltpu.VMEM((BLOCK, KV), F32),
            pltpu.VMEM((BLOCK, 128), F32),
            pltpu.VMEM((BLOCK, 128), F32),
            pltpu.VMEM((OWN, ROWS, 7 * 128), F32),
            pltpu.VMEM((PAIRS, 4, BLOCK, 128), F32),
            pltpu.VMEM((PAIRS, BLOCK, 128), BF16),
            pltpu.VMEM((PAIRS, BLOCK, 128), BF16),
            pltpu.VMEM((OWN, BLOCK, 128), BF16),
            pltpu.VMEM((PAIRS, BLOCK, 256), BF16),
            pltpu.VMEM((BLOCK, 256), BF16),
            pltpu.VMEM((2, PAIRS, 128, 128), BF16),
            pltpu.VMEM((SIDE, PAIRS, 128, 128), BF16),
            pltpu.VMEM((PAIRS, 256, 256), BF16),
            pltpu.VMEM((SIDE, ROWS, 512), F32),
            pltpu.VMEM((3, ROWS, 512), BF16),
            pltpu.VMEM((2, 64, 512), BF16),
            pltpu.VMEM((SIDE, ROWS, 512), BF16),
            pltpu.VMEM((ROWS, D), F32),
            dma((9,)), dma((6,)), dma((6,)),
            dma((2, 4)), dma((2, 4)), dma((8,)), dma((8,)),
            dma((2, 4)), dma((2, 4)), dma((8,)), dma((8,)),
            dma((2, 4)), dma((2, 4)),
            dma((8, 2)), dma((8, 2)), dma((8, 2)), dma((8, 2)),
            dma((8, 4)), dma((8, 4)), dma((1,)), dma((1,)),
            dma((2, 4)), dma((2, 4)), dma((8,)), dma((8,)),
            dma((3,)), dma((3,)), dma((6,)), dma((6,)), dma((4,)), dma((4,)),
        ],
        compiler_params=pltpu.CompilerParams(
            collective_id=0, has_side_effects=True, vmem_limit_bytes=60 * 1024 * 1024
        ),
        name="retention",
    )(
        tokens, query_weight, key_weight, value_weight, output_weight, log_decay.T, frequency
    )


def solution(mesh):
    placed = (
        P("dp", "sp", None),
        P("dp", None),
        P("dp", None),
        P("dp", None),
        P("dp", None),
        P(None, "sp"),
    )
    return jax.shard_map(
        shards, mesh=mesh, in_specs=placed, out_specs=P("dp", "sp", None), check_vma=False
    )
```

```python
import jax
import jax.numpy as jnp
import numpy as np
from jax import lax
from jax.experimental import pallas as pl
from jax.experimental.pallas import tpu as pltpu
from jax.sharding import PartitionSpec as P

D = 2048
HEADS = 16
DK = 64
DV = 128
BLOCK = 512
ROWS = 128
SIDE = 4
RING = 8
OWN = 4
PAIRS = 2
EPS = 1e-6
KV = 768
PART = 384
REST = 512

F32 = jnp.float32
BF16 = jnp.bfloat16


def mod(value, size):
    return lax.rem(value + size, size)


def matmul(a, b):
    return jnp.dot(a, b, preferred_element_type=F32)


def kernel(
    tok_hbm, q_hbm, k_hbm, v_hbm, o_hbm, ld_hbm, freq_hbm, out_ref,
    tok, wq, wk, wo, wz, ld_ref, freq_ref, own_rate, rates, acc_q, acc_k, cosine, sine, tiles, decay, qr, kr, vb, qs, ks,
    ab, states, carried, ret, ns, relay, nb, acc_o,
    local_sem, tok_s, tok_r, wq_s, wq_r, wqd_s, wqd_r, wk_s, wk_r, wkd_s, wkd_r, wo_s, wo_r,
    wy_s, wy_r, wf_s, wf_r, wod_s, wod_r, own_s, own_r, wz_s, wz_r, wzd_s, wzd_r, st_s, st_r, nb_s, nb_r, ld_s, ld_r,
):
    sp = lax.axis_index("sp")
    dp = lax.axis_index("dp")
    y, x = lax.div(sp, SIDE), lax.rem(sp, SIDE)
    z, c = lax.div(dp, 2), lax.rem(dp, 2)
    right, left, across = mod(x + 1, SIDE), mod(x - 1, SIDE), mod(x + 2, SIDE)
    above, below, facing = mod(y + 1, SIDE), mod(y - 1, SIDE), mod(y + 2, SIDE)
    h0, h1 = pl.ds(0, 64), pl.ds(64, 64)

    def at_x(to):
        return (y * SIDE + to, dp)

    def at_y(to):
        return (to * SIDE + x, dp)

    def at_z(to):
        return (sp, to * 2 + c)

    other_core = (sp, z * 2 + (1 - c))
    sends = []

    def send(src, dst, send_sem, recv_sem, to):
        copy = pltpu.make_async_remote_copy(
            src_ref=src, dst_ref=dst, send_sem=send_sem, recv_sem=recv_sem,
            device_id=to, device_id_type=pl.DeviceIdType.MESH,
        )
        copy.start()
        sends.append(copy)

    def arrive(dst, send_sem, recv_sem):
        pltpu.make_async_remote_copy(
            src_ref=dst, dst_ref=dst, send_sem=send_sem, recv_sem=recv_sem,
            device_id=other_core, device_id_type=pl.DeviceIdType.MESH,
        ).wait_recv()

    fetched = []

    def fetch(src, dst):
        copy = pltpu.make_async_copy(src, dst, local_sem.at[len(fetched)])
        copy.start()
        fetched.append(copy)

    fetch(ld_hbm, ld_ref)
    fetch(k_hbm.at[:, pl.ds(pl.multiple_of(x * 256, 256), 256)], wk.at[dp, :, 0:256])
    fetch(v_hbm.at[:, pl.ds(pl.multiple_of(x * 512, 512), 512)], wk.at[dp, :, 256:KV])
    fetch(tok_hbm.at[0], tok.at[x])
    for part in range(SIDE):
        fetch(o_hbm.at[:, part * PART:(part + 1) * PART], wo.at[part, dp])
    fetch(q_hbm.at[:, pl.ds(pl.multiple_of(x * 256, 256), 256)], wq.at[dp])
    fetch(freq_hbm, freq_ref)
    fetch(o_hbm.at[:, SIDE * PART:D], wz.at[dp])
    needed = {"LD": (0,), "K0": (1, 2), "T0": (3,), "O0": (4, 5, 6, 7), "Q0": (8,), "TAB": (9,), "Z0": (10,)}

    barrier = pltpu.get_barrier_semaphore()
    peers = [(lax.rem(sp + o, SIDE * SIDE), dp) for o in range(1, SIDE * SIDE)]
    peers += [at_z(mod(z + 1, RING)), at_z(mod(z - 1, RING)), other_core]
    for peer in peers:
        pl.semaphore_signal(
            barrier, inc=1, device_id=peer, device_id_type=pl.DeviceIdType.MESH
        )
    pl.semaphore_wait(barrier, len(peers))

    def half(direction):
        return h0 if direction == 0 else h1

    def z_block(direction, step):
        return mod(z - step if direction == 0 else z + step, RING) * 2 + c

    def z_next(direction):
        return mod(z + 1 if direction == 0 else z - 1, RING)

    def nth_block(n):
        if n == 0:
            return dp
        if n == 7:
            return z_block(0, 4)
        return z_block((n - 1) % 2, (n + 1) // 2)

    def nth_other(n):
        return nth_block(n) + 1 - 2 * c

    def blocks_of(step):
        return (0,) if step == 0 else (2 * step - 1, 2 * step) if step < 4 else (7,)

    def ring_wait(view, step, s_sem, r_sem):
        if step > 0:
            for d in range(2):
                b = z_block(d, step)
                arrive(
                    view(b) if step < 4 else view(b, half(d)), s_sem.at[d, step - 1], r_sem.at[d, step - 1]
                )

    def ring_send(view, step, s_sem, r_sem):
        if step < 4:
            for d in range(2):
                b = z_block(d, step)
                part = view(b) if step < 3 else view(b, half(d))
                send(part, part, s_sem.at[d, step], r_sem.at[d, step], at_z(z_next(d)))

    def weight_step(ref, step, s_sem, r_sem, d_s, d_r):
        def view(b, rows=None):
            return ref.at[b] if rows is None else ref.at[b, rows]

        ring_wait(view, step, s_sem, r_sem)
        ring_send(view, step, s_sem, r_sem)
        for n in blocks_of(step):
            b = nth_block(n)
            send(ref.at[b], ref.at[b], d_s.at[n], d_r.at[n], other_core)

    def k_step(step):
        weight_step(wk, step, wk_s, wk_r, wkd_s, wkd_r)

    def q_step(step):
        weight_step(wq, step, wq_s, wq_r, wqd_s, wqd_r)

    def zz_step(step):
        weight_step(wz, step, wz_s, wz_r, wzd_s, wzd_r)

    def share(part, n, index):
        send(part, part, wod_s.at[n, index], wod_r.at[n, index], other_core)

    def o_step(step):
        def view(b, rows=None):
            return wo.at[y, b] if rows is None else wo.at[y, b, rows]

        ring_wait(view, step, wo_s, wo_r)
        ring_send(view, step, wo_s, wo_r)
        if step > 0:
            for n in blocks_of(step):
                part = wo.at[y, nth_block(n)]
                send(part, part, wy_s.at[n, 0], wy_r.at[n, 0], at_y(above))
                send(part, part, wy_s.at[n, 1], wy_r.at[n, 1], at_y(below))

    def f_step(step):
        for n in blocks_of(step):
            b = nth_block(n)
            arrive(wo.at[below, b], wy_s.at[n, 0], wy_r.at[n, 0])
            arrive(wo.at[above, b], wy_s.at[n, 1], wy_r.at[n, 1])
            up, down = wo.at[below, b, h0], wo.at[above, b, h1]
            send(up, up, wf_s.at[n, 0], wf_r.at[n, 0], at_y(above))
            send(down, down, wf_s.at[n, 1], wf_r.at[n, 1], at_y(below))

    def d_step(step):
        for n in blocks_of(step):
            for index, part in enumerate((y, below, above)):
                share(wo.at[part, nth_block(n)], n, index)

    def g_step(step):
        for n in blocks_of(step):
            b = nth_block(n)
            arrive(wo.at[facing, b, h0], wf_s.at[n, 0], wf_r.at[n, 0])
            arrive(wo.at[facing, b, h1], wf_s.at[n, 1], wf_r.at[n, 1])
            share(wo.at[facing, b], n, 3)

    def own_output_block():
        send(wo.at[:, dp], wo.at[:, dp], own_s.at[0], own_r.at[0], other_core)

    def take_output(n):
        b = nth_other(n)
        if n == 0:
            arrive(wo.at[:, b], own_s.at[0], own_r.at[0])
        else:
            for index, part in enumerate((y, below, above, facing)):
                arrive(wo.at[part, b], wod_s.at[n, index], wod_r.at[n, index])

    def tokens_first():
        send(tok.at[x, h0], tok.at[x, h0], tok_s.at[0], tok_r.at[0], at_x(right))
        send(tok.at[x, h1], tok.at[x, h1], tok_s.at[1], tok_r.at[1], at_x(left))

    def tokens_second():
        send(tok.at[x, h1], tok.at[x, h1], tok_s.at[2], tok_r.at[2], at_x(right))
        send(tok.at[x, h0], tok.at[x, h0], tok_s.at[3], tok_r.at[3], at_x(left))

    def tokens_forward():
        arrive(tok.at[left, h0], tok_s.at[0], tok_r.at[0])
        send(tok.at[left, h0], tok.at[left, h0], tok_s.at[4], tok_r.at[4], at_x(right))
        arrive(tok.at[right, h1], tok_s.at[1], tok_r.at[1])
        send(tok.at[right, h1], tok.at[right, h1], tok_s.at[5], tok_r.at[5], at_x(left))

    def rate_copy(to):
        return pltpu.make_async_remote_copy(
            src_ref=own_rate, dst_ref=rates.at[x], send_sem=ld_s.at[to], recv_sem=ld_r.at[x],
            device_id=(to * SIDE + y, dp), device_id_type=pl.DeviceIdType.MESH,
        )

    def send_rates():
        sub = lax.broadcasted_iota(jnp.int32, (8, 128), 0)
        own_rate[...] = jnp.where(sub == 0, ld_ref[0:1, 0:1], ld_ref[0:1, 1:2])
        for to in range(SIDE):
            @pl.when(jnp.logical_or(y != x, y != to))
            def _():
                rate_copy(to).start()

            @pl.when(jnp.logical_and(y == x, y == to))
            def _():
                pltpu.make_async_copy(own_rate, rates.at[x], ld_r.at[x]).start()

    lane = lax.broadcasted_iota(jnp.int32, (1, 128), 1)
    low = lax.rem(lane, 64) < 32

    def tables():
        for part in range(SIDE):
            rows = pl.ds(part * ROWS, ROWS)
            at = lax.broadcasted_iota(jnp.int32, (ROWS, 128), 0) + (y * BLOCK + part * ROWS)
            angle = at.astype(F32) * freq_ref[...]
            cosine[rows, :] = jnp.cos(angle)
            turned = jnp.sin(angle)
            sine[rows, :] = jnp.where(low, -turned, turned)

    def decays():
        for j in range(SIDE):
            arrive(rates.at[j], ld_s.at[j], ld_r.at[j])

        def decay_tiles(h, carry):
            a, b = rates[h, 0:1, :], rates[h, 1:2, :]
            i = lax.broadcasted_iota(jnp.int32, (ROWS, 128), 0)
            j = lax.broadcasted_iota(jnp.int32, (ROWS, 128), 1)
            for m in range(7):
                apart = (i - j + (3 - m) * ROWS).astype(F32)
                rate = jnp.where(apart >= 0.0, a, b)
                value = jnp.exp(rate * jnp.abs(apart))
                tiles[h, :, m * 128:(m + 1) * 128] = jnp.where(apart == 0.0, 2.0, value)
            return carry

        lax.fori_loop(0, OWN, decay_tiles, 0)
        first_head = lane < 64

        def decay_rows(p, carry):
            a = jnp.where(first_head, rates[2 * p, 0:1, :], rates[2 * p + 1, 0:1, :])
            b = jnp.where(first_head, rates[2 * p, 1:2, :], rates[2 * p + 1, 1:2, :])
            t = lax.broadcasted_iota(jnp.int32, (BLOCK, 128), 0).astype(F32)
            decay[p, 0] = jnp.exp((t + 1.0) * a)
            decay[p, 1] = jnp.exp((BLOCK - t) * b)
            decay[p, 2] = jnp.exp((BLOCK - 1.0 - t) * a)
            decay[p, 3] = jnp.exp(t * b)
            return carry

        lax.fori_loop(0, PAIRS, decay_rows, 0)

    def tokens_all():
        arrive(tok.at[left, h1], tok_s.at[2], tok_r.at[2])
        arrive(tok.at[right, h0], tok_s.at[3], tok_r.at[3])
        arrive(tok.at[across, h0], tok_s.at[4], tok_r.at[4])
        arrive(tok.at[across, h1], tok_s.at[5], tok_r.at[5])

    def project(ref, acc, width, offset, fresh):
        at = mod(z + offset, RING)
        rows = tok[:, :, pl.ds(pl.multiple_of(at * 256, 256), 256)].reshape(BLOCK, 256)
        for n in range(width // 256):
            cols = slice(n * 256, (n + 1) * 256)
            part = matmul(rows, ref[pl.ds(at * 2, 2), :, cols].reshape(256, 256))
            acc[:, cols] = part if fresh else acc[:, cols] + part

    def project_many(ref, acc, width, first, count, stride):
        def step(i, carry):
            project(ref, acc, width, first + i * stride, False)
            return carry

        lax.fori_loop(0, count, step, 0)

    def k_project(stage):
        k_or_q(stage, wk, acc_k, KV, wkd_s, wkd_r)

    def q_project(stage):
        k_or_q(stage, wq, acc_q, 256, wqd_s, wqd_r)

    def k_or_q(stage, ref, acc, width, d_s, d_r):
        for n in ((0, 1, 2), (3, 4), (5, 6), (7,))[stage]:
            arrive(ref.at[nth_other(n)], d_s.at[n], d_r.at[n])
        if stage == 0:
            project(ref, acc, width, 0, True)
            project_many(ref, acc, width, 1, 2, 6)
        elif stage == 3:
            project(ref, acc, width, 4, False)
        else:
            project_many(ref, acc, width, stage + 1, 2, 6 - 2 * stage)

    def turn(flat):
        wide = flat.astype(BF16).astype(F32)
        partner = jnp.where(low, pltpu.roll(wide, 96, 1), pltpu.roll(wide, 32, 1))
        return (wide * cosine[...] + partner * sine[...]).astype(BF16)

    row_low = lax.broadcasted_iota(jnp.int32, (128, 1), 0) < 64

    def keys_values():
        for p in range(PAIRS):
            rk = turn(acc_k[:, p * 128:(p + 1) * 128])
            kr[p] = rk
            value = acc_k[:, 256 + p * 256:256 + (p + 1) * 256].astype(BF16)
            vb[2 * p] = value[:, :128]
            vb[2 * p + 1] = value[:, 128:]
            wide_k = rk.astype(F32)
            ks[:, 0:128] = (wide_k * decay[p, 2]).astype(BF16)
            ks[:, 128:256] = (wide_k * decay[p, 3]).astype(BF16)
            both = lax.dot_general(
                ks[...], value, (((0,), (0,)), ((), ())), preferred_element_type=F32
            )
            for d in range(2):
                square = both[d * 128:(d + 1) * 128]
                ab[d, p] = jnp.where(row_low, square[:, :128], square[:, 128:]).astype(BF16)
        for n, to in ((2, facing), (0, above), (1, below)):
            send(ab.at[jnp.where(to > y, 0, 1)], states.at[y], st_s.at[n], st_r.at[n], at_y(to))

    def queries():
        for p in range(PAIRS):
            rq = turn(acc_q[:, p * 128:(p + 1) * 128])
            qr[p] = rq
            wide_q = rq.astype(F32)
            qs[p, :, 0:128] = (wide_q * decay[p, 0]).astype(BF16)
            qs[p, :, 128:256] = (wide_q * decay[p, 1]).astype(BF16)

    def in_block(r):
        rows = pl.ds(pl.multiple_of(r * ROWS, ROWS), ROWS)
        cols = pl.ds(pl.multiple_of((3 - r) * 128, 128), BLOCK)
        for h in range(OWN):
            query = jnp.where((lane >= 64) == (h % 2 == 1), qr[h // 2, rows, :], jnp.zeros((), BF16))
            scores = lax.dot_general(
                query, kr[h // 2], (((1,), (1,)), ((), ())), preferred_element_type=F32
            )
            scores = (scores * tiles[h, :, cols]).astype(BF16)
            ret[r, :, h * 128:(h + 1) * 128] = matmul(scores, vb[h])

    def carry_states():
        arrive(states.at[below], st_s.at[0], st_r.at[0])
        arrive(states.at[above], st_s.at[1], st_r.at[1])
        arrive(states.at[facing], st_s.at[2], st_r.at[2])
        for p in range(PAIRS):
            for d in range(2):
                rate = jnp.where(row_low, rates[2 * p, d:d + 1, 0:1], rates[2 * p + 1, d:d + 1, 0:1])
                total = jnp.zeros((128, 128), F32)
                for o in range(1, SIDE):
                    source = mod(y - o if d == 0 else y + o, SIDE)
                    there = (y - o >= 0) if d == 0 else (y + o < SIDE)
                    weight = jnp.exp(rate * (BLOCK * (o - 1.0)))
                    total = total + jnp.where(there, weight * states[source, p].astype(F32), 0.0)
                total = total.astype(BF16)
                zero = jnp.zeros((), BF16)
                carried[p, d * 128:(d + 1) * 128, 0:128] = jnp.where(row_low, total, zero)
                carried[p, d * 128:(d + 1) * 128, 128:256] = jnp.where(row_low, zero, total)

    def finish_rows(r, dst):
        rows = pl.ds(pl.multiple_of(r * ROWS, ROWS), ROWS)
        for p in range(PAIRS):
            outside = matmul(qs[p, rows, :], carried[p])
            for e in range(2):
                h = 2 * p + e
                whole = ret[r, :, h * 128:(h + 1) * 128] + outside[:, e * 128:(e + 1) * 128]
                centred = whole - jnp.mean(whole, axis=-1, keepdims=True)
                var = jnp.mean(centred * centred, axis=-1, keepdims=True)
                dst[:, h * 128:(h + 1) * 128] = (centred * lax.rsqrt(var + EPS)).astype(BF16)

    to_rows = (across, left, right, x)

    def normed(n):
        r = to_rows[n]
        if n == 3:
            finish_rows(r, nb.at[x])
            return
        finish_rows(r, ns.at[n])
        if n == 0:
            send(ns.at[0, h0], relay.at[0], nb_s.at[0], nb_r.at[0], at_x(right))
            send(ns.at[0, h1], relay.at[1], nb_s.at[1], nb_r.at[1], at_x(left))
        else:
            send(ns.at[n], nb.at[x], nb_s.at[n + 1], nb_r.at[n + 1], at_x(r))

    def normed_forward():
        arrive(relay.at[0], nb_s.at[0], nb_r.at[0])
        send(relay.at[0], nb.at[left, h0], nb_s.at[4], nb_r.at[4], at_x(right))
        arrive(relay.at[1], nb_s.at[1], nb_r.at[1])
        send(relay.at[1], nb.at[right, h1], nb_s.at[5], nb_r.at[5], at_x(left))

    def normed_all():
        arrive(nb.at[right], nb_s.at[2], nb_r.at[2])
        arrive(nb.at[left], nb_s.at[3], nb_r.at[3])
        arrive(nb.at[across, h0], nb_s.at[4], nb_r.at[4])
        arrive(nb.at[across, h1], nb_s.at[5], nb_r.at[5])

    def output(stage):
        if stage == 0:
            normed_all()
        for n in ((0, 1, 2, 3, 4), (5, 6, 7))[stage]:
            take_output(n)
            arrive(wz.at[nth_other(n)], wzd_s.at[n], wzd_r.at[n])
        offsets = ((0, 1, 7, 2, 6), (3, 5, 4))[stage]
        left_hand, blocks = [], []
        for offset in offsets:
            at = mod(z + offset, RING)
            start = pl.multiple_of(lax.rem(at, 2) * 256, 256)
            left_hand.append(nb[lax.div(at, 2), :, pl.ds(start, 256)])
            blocks.append(pl.ds(at * 2, 2))
        for part in range(SIDE + 1):
            width = PART if part < SIDE else REST
            cols = slice(part * PART, part * PART + width)
            total = jnp.zeros((ROWS, width), F32) if stage == 0 else acc_o[:, cols]
            for lhs, rows in zip(left_hand, blocks):
                weight = wo[part, rows] if part < SIDE else wz[rows]
                total = total + matmul(lhs, weight.reshape(256, width))
            if stage == 0:
                acc_o[:, cols] = total
            else:
                out_ref[0, :, cols] = total.astype(BF16)

    def run(name, task, *arguments):
        with jax.named_scope(name):
            for n in needed.get(name, ()):
                fetched[n].wait()
            task(*arguments)

    run("K0", k_step, 0)
    run("T0", tokens_first)
    run("LD", send_rates)
    run("T1", tokens_second)
    run("O0", o_step, 0)
    run("TAB", tables)
    run("K1", k_step, 1)
    run("Q0", q_step, 0)
    run("TF", tokens_forward)
    run("O1", o_step, 1)
    run("K2", k_step, 2)
    run("Q1", q_step, 1)
    run("O2", o_step, 2)
    run("F1", f_step, 1)
    run("TA", tokens_all)
    run("KA", k_project, 0)
    run("K3", k_step, 3)
    run("QA", q_project, 0)
    run("Q2", q_step, 2)
    run("SO0", own_output_block)
    run("Z0", zz_step, 0)
    run("F2", f_step, 2)
    run("KB", k_project, 1)
    run("D1", d_step, 1)
    run("O3", o_step, 3)
    run("QB", q_project, 1)
    run("G1", g_step, 1)
    run("K4", k_step, 4)
    run("DEC", decays)
    run("D2", d_step, 2)
    run("G2", g_step, 2)
    run("Q3", q_step, 3)
    run("KC", k_project, 2)
    run("KD", k_project, 3)
    run("RK", keys_values)
    run("Z1", zz_step, 1)
    run("O4", o_step, 4)
    run("F3", f_step, 3)
    run("QC", q_project, 2)
    run("Q4", q_step, 4)
    run("QD", q_project, 3)
    run("RQ", queries)
    run("I2", in_block, to_rows[2])
    run("Z2", zz_step, 2)
    run("I0", in_block, to_rows[0])
    run("CAR", carry_states)
    run("N0", normed, 0)
    run("I1", in_block, to_rows[1])
    run("N1", normed, 1)
    run("N2", normed, 2)
    run("F4", f_step, 4)
    run("I3", in_block, to_rows[3])
    run("D4", d_step, 4)
    run("D3", d_step, 3)
    run("Z3", zz_step, 3)
    run("NF", normed_forward)
    run("G3", g_step, 3)
    run("G4", g_step, 4)
    run("Z4", zz_step, 4)
    run("N3", normed, 3)
    run("OA", output, 0)
    run("OB", output, 1)
    for copy in sends:
        copy.wait_send()
    for to in range(SIDE):
        @pl.when(jnp.logical_or(y != x, y != to))
        def _():
            rate_copy(to).wait_send()


def shards(tokens, query_weight, key_weight, value_weight, output_weight, log_decay):
    half_dim = DK // 2
    frequency = (
        np.float32(10000.0) ** (-np.arange(half_dim, dtype=np.float32) / np.float32(half_dim))
    ).astype(np.float32)
    frequency = jnp.asarray(np.tile(frequency, 4)[None, :])
    anywhere = pl.BlockSpec(memory_space=pl.ANY)
    vmem = pl.BlockSpec(memory_space=pltpu.VMEM)
    dma = pltpu.SemaphoreType.DMA
    return pl.pallas_call(
        kernel,
        out_shape=pltpu.VMEM((1, ROWS, D), BF16),
        in_specs=[anywhere] * 7,
        out_specs=vmem,
        scratch_shapes=[
            pltpu.VMEM((SIDE, ROWS, D), BF16),
            pltpu.VMEM((16, 128, 256), BF16),
            pltpu.VMEM((16, 128, KV), BF16),
            pltpu.VMEM((SIDE, 16, 128, PART), BF16),
            pltpu.VMEM((16, 128, REST), BF16),
            pltpu.VMEM((1, 2), F32),
            pltpu.VMEM((1, 128), F32),
            pltpu.VMEM((8, 128), F32),
            pltpu.VMEM((SIDE, 8, 128), F32),
            pltpu.VMEM((BLOCK, 256), F32),
            pltpu.VMEM((BLOCK, KV), F32),
            pltpu.VMEM((BLOCK, 128), F32),
            pltpu.VMEM((BLOCK, 128), F32),
            pltpu.VMEM((OWN, ROWS, 7 * 128), F32),
            pltpu.VMEM((PAIRS, 4, BLOCK, 128), F32),
            pltpu.VMEM((PAIRS, BLOCK, 128), BF16),
            pltpu.VMEM((PAIRS, BLOCK, 128), BF16),
            pltpu.VMEM((OWN, BLOCK, 128), BF16),
            pltpu.VMEM((PAIRS, BLOCK, 256), BF16),
            pltpu.VMEM((BLOCK, 256), BF16),
            pltpu.VMEM((2, PAIRS, 128, 128), BF16),
            pltpu.VMEM((SIDE, PAIRS, 128, 128), BF16),
            pltpu.VMEM((PAIRS, 256, 256), BF16),
            pltpu.VMEM((SIDE, ROWS, 512), F32),
            pltpu.VMEM((3, ROWS, 512), BF16),
            pltpu.VMEM((2, 64, 512), BF16),
            pltpu.VMEM((SIDE, ROWS, 512), BF16),
            pltpu.VMEM((ROWS, D), F32),
            dma((11,)), dma((6,)), dma((6,)),
            dma((2, 4)), dma((2, 4)), dma((8,)), dma((8,)),
            dma((2, 4)), dma((2, 4)), dma((8,)), dma((8,)),
            dma((2, 4)), dma((2, 4)),
            dma((8, 2)), dma((8, 2)), dma((8, 2)), dma((8, 2)),
            dma((8, 4)), dma((8, 4)), dma((1,)), dma((1,)),
            dma((2, 4)), dma((2, 4)), dma((8,)), dma((8,)),
            dma((3,)), dma((3,)), dma((6,)), dma((6,)), dma((4,)), dma((4,)),
        ],
        compiler_params=pltpu.CompilerParams(
            collective_id=0, has_side_effects=True, vmem_limit_bytes=60 * 1024 * 1024
        ),
        name="retention",
    )(
        tokens, query_weight, key_weight, value_weight, output_weight, log_decay.T, frequency
    )


def solution(mesh):
    placed = (
        P("dp", "sp", None),
        P("dp", None),
        P("dp", None),
        P("dp", None),
        P("dp", None),
        P(None, "sp"),
    )
    return jax.shard_map(
        shards, mesh=mesh, in_specs=placed, out_specs=P("dp", "sp", None), check_vma=False
    )
```

```python
import jax
import jax.numpy as jnp
import numpy as np
from jax import lax
from jax.experimental import pallas as pl
from jax.experimental.pallas import tpu as pltpu
from jax.sharding import PartitionSpec as P

D = 2048
HEADS = 16
DK = 64
DV = 128
BLOCK = 512
ROWS = 128
SIDE = 4
RING = 8
OWN = 4
PAIRS = 2
EPS = 1e-6
KV = 768
PART = 384
REST = 512

F32 = jnp.float32
BF16 = jnp.bfloat16


def mod(value, size):
    return lax.rem(value + size, size)


def matmul(a, b):
    return jnp.dot(a, b, preferred_element_type=F32)


def kernel(
    tok_hbm, q_hbm, k_hbm, v_hbm, o_hbm, ld_hbm, freq_hbm, out_ref,
    tok, wq, wk, wo, wz, ld_ref, freq_ref, own_rate, rates, acc_q, acc_k, cosine, sine, tiles, decay, qr, kr, vb, qs, ks,
    ab, states, carried, ret, ns, relay, nb, acc_o,
    local_sem, tok_s, tok_r, wq_s, wq_r, wqd_s, wqd_r, wk_s, wk_r, wkd_s, wkd_r, wo_s, wo_r,
    wy_s, wy_r, wf_s, wf_r, wod_s, wod_r, own_s, own_r, wz_s, wz_r, wzd_s, wzd_r, st_s, st_r, nb_s, nb_r, ld_s, ld_r, lr_r,
):
    sp = lax.axis_index("sp")
    dp = lax.axis_index("dp")
    y, x = lax.div(sp, SIDE), lax.rem(sp, SIDE)
    z, c = lax.div(dp, 2), lax.rem(dp, 2)
    right, left, across = mod(x + 1, SIDE), mod(x - 1, SIDE), mod(x + 2, SIDE)
    above, below, facing = mod(y + 1, SIDE), mod(y - 1, SIDE), mod(y + 2, SIDE)
    h0, h1 = pl.ds(0, 64), pl.ds(64, 64)

    def at_x(to):
        return (y * SIDE + to, dp)

    def at_y(to):
        return (to * SIDE + x, dp)

    def at_z(to):
        return (sp, to * 2 + c)

    other_core = (sp, z * 2 + (1 - c))
    sends = []

    def send(src, dst, send_sem, recv_sem, to):
        copy = pltpu.make_async_remote_copy(
            src_ref=src, dst_ref=dst, send_sem=send_sem, recv_sem=recv_sem,
            device_id=to, device_id_type=pl.DeviceIdType.MESH,
        )
        copy.start()
        sends.append(copy)

    def arrive(dst, send_sem, recv_sem):
        pltpu.make_async_remote_copy(
            src_ref=dst, dst_ref=dst, send_sem=send_sem, recv_sem=recv_sem,
            device_id=other_core, device_id_type=pl.DeviceIdType.MESH,
        ).wait_recv()

    fetched = []

    def fetch(src, dst):
        copy = pltpu.make_async_copy(src, dst, local_sem.at[len(fetched)])
        copy.start()
        fetched.append(copy)

    fetch(k_hbm.at[:, pl.ds(pl.multiple_of(x * 256, 256), 256)], wk.at[dp, :, 0:256])
    fetch(v_hbm.at[:, pl.ds(pl.multiple_of(x * 512, 512), 512)], wk.at[dp, :, 256:KV])

    barrier = pltpu.get_barrier_semaphore()
    peers = [at_z(mod(z + 1, RING)), at_z(mod(z - 1, RING)), other_core]
    peers += [at_x(to) for to in (right, left, across)] + [at_y(to) for to in (above, below, facing)]
    for peer in peers:
        pl.semaphore_signal(
            barrier, inc=1, device_id=peer, device_id_type=pl.DeviceIdType.MESH
        )
    fetch(tok_hbm.at[0], tok.at[x])
    fetch(ld_hbm, ld_ref)
    for part in range(SIDE):
        fetch(o_hbm.at[:, part * PART:(part + 1) * PART], wo.at[part, dp])
    fetch(q_hbm.at[:, pl.ds(pl.multiple_of(x * 256, 256), 256)], wq.at[dp])
    fetch(freq_hbm, freq_ref)
    fetch(o_hbm.at[:, SIDE * PART:D], wz.at[dp])
    needed = {"K0": (0, 1), "T0": (2,), "LD": (3,), "O0": (4, 5, 6, 7), "Q0": (8,), "TAB": (9,), "Z0": (10,)}
    pl.semaphore_wait(barrier, len(peers))

    def half(direction):
        return h0 if direction == 0 else h1

    def z_block(direction, step):
        return mod(z - step if direction == 0 else z + step, RING) * 2 + c

    def z_next(direction):
        return mod(z + 1 if direction == 0 else z - 1, RING)

    def nth_block(n):
        if n == 0:
            return dp
        if n == 7:
            return z_block(0, 4)
        return z_block((n - 1) % 2, (n + 1) // 2)

    def nth_other(n):
        return nth_block(n) + 1 - 2 * c

    def blocks_of(step):
        return (0,) if step == 0 else (2 * step - 1, 2 * step) if step < 4 else (7,)

    def ring_wait(view, step, s_sem, r_sem):
        if step > 0:
            for d in range(2):
                b = z_block(d, step)
                arrive(
                    view(b) if step < 4 else view(b, half(d)), s_sem.at[d, step - 1], r_sem.at[d, step - 1]
                )

    def ring_send(view, step, s_sem, r_sem):
        if step < 4:
            for d in range(2):
                b = z_block(d, step)
                part = view(b) if step < 3 else view(b, half(d))
                send(part, part, s_sem.at[d, step], r_sem.at[d, step], at_z(z_next(d)))

    def weight_step(ref, step, s_sem, r_sem, d_s, d_r):
        def view(b, rows=None):
            return ref.at[b] if rows is None else ref.at[b, rows]

        ring_wait(view, step, s_sem, r_sem)
        ring_send(view, step, s_sem, r_sem)
        for n in blocks_of(step):
            b = nth_block(n)
            send(ref.at[b], ref.at[b], d_s.at[n], d_r.at[n], other_core)

    def k_step(step):
        weight_step(wk, step, wk_s, wk_r, wkd_s, wkd_r)

    def q_step(step):
        weight_step(wq, step, wq_s, wq_r, wqd_s, wqd_r)

    def zz_step(step):
        weight_step(wz, step, wz_s, wz_r, wzd_s, wzd_r)

    def share(part, n, index):
        send(part, part, wod_s.at[n, index], wod_r.at[n, index], other_core)

    def o_step(step):
        def view(b, rows=None):
            return wo.at[y, b] if rows is None else wo.at[y, b, rows]

        ring_wait(view, step, wo_s, wo_r)
        ring_send(view, step, wo_s, wo_r)
        if step > 0:
            for n in blocks_of(step):
                part = wo.at[y, nth_block(n)]
                send(part, part, wy_s.at[n, 0], wy_r.at[n, 0], at_y(above))
                send(part, part, wy_s.at[n, 1], wy_r.at[n, 1], at_y(below))

    def f_step(step):
        for n in blocks_of(step):
            b = nth_block(n)
            arrive(wo.at[below, b], wy_s.at[n, 0], wy_r.at[n, 0])
            arrive(wo.at[above, b], wy_s.at[n, 1], wy_r.at[n, 1])
            up, down = wo.at[below, b, h0], wo.at[above, b, h1]
            send(up, up, wf_s.at[n, 0], wf_r.at[n, 0], at_y(above))
            send(down, down, wf_s.at[n, 1], wf_r.at[n, 1], at_y(below))

    def d_step(step):
        for n in blocks_of(step):
            for index, part in enumerate((y, below, above)):
                share(wo.at[part, nth_block(n)], n, index)

    def g_step(step):
        for n in blocks_of(step):
            b = nth_block(n)
            arrive(wo.at[facing, b, h0], wf_s.at[n, 0], wf_r.at[n, 0])
            arrive(wo.at[facing, b, h1], wf_s.at[n, 1], wf_r.at[n, 1])
            share(wo.at[facing, b], n, 3)

    def own_output_block():
        send(wo.at[:, dp], wo.at[:, dp], own_s.at[0], own_r.at[0], other_core)

    def take_output(n):
        b = nth_other(n)
        if n == 0:
            arrive(wo.at[:, b], own_s.at[0], own_r.at[0])
        else:
            for index, part in enumerate((y, below, above, facing)):
                arrive(wo.at[part, b], wod_s.at[n, index], wod_r.at[n, index])

    def tokens_first():
        send(tok.at[x, h0], tok.at[x, h0], tok_s.at[0], tok_r.at[0], at_x(right))
        send(tok.at[x, h1], tok.at[x, h1], tok_s.at[1], tok_r.at[1], at_x(left))

    def tokens_second():
        send(tok.at[x, h1], tok.at[x, h1], tok_s.at[2], tok_r.at[2], at_x(right))
        send(tok.at[x, h0], tok.at[x, h0], tok_s.at[3], tok_r.at[3], at_x(left))

    def tokens_forward():
        arrive(tok.at[left, h0], tok_s.at[0], tok_r.at[0])
        send(tok.at[left, h0], tok.at[left, h0], tok_s.at[4], tok_r.at[4], at_x(right))
        arrive(tok.at[right, h1], tok_s.at[1], tok_r.at[1])
        send(tok.at[right, h1], tok.at[right, h1], tok_s.at[5], tok_r.at[5], at_x(left))

    def rate_copy():
        return pltpu.make_async_remote_copy(
            src_ref=own_rate, dst_ref=rates.at[x], send_sem=ld_s.at[0], recv_sem=ld_r.at[x],
            device_id=at_x(y), device_id_type=pl.DeviceIdType.MESH,
        )

    def rates_copy(n, to):
        return pltpu.make_async_remote_copy(
            src_ref=rates, dst_ref=rates, send_sem=ld_s.at[n], recv_sem=lr_r.at[0],
            device_id=at_y(to), device_id_type=pl.DeviceIdType.MESH,
        )

    def send_rates():
        sub = lax.broadcasted_iota(jnp.int32, (8, 128), 0)
        own_rate[...] = jnp.where(sub == 0, ld_ref[0:1, 0:1], ld_ref[0:1, 1:2])

        @pl.when(x != y)
        def _():
            rate_copy().start()

        @pl.when(x == y)
        def _():
            pltpu.make_async_copy(own_rate, rates.at[x], ld_r.at[x]).start()

    def forward_rates():
        @pl.when(x == y)
        def _():
            for j in range(SIDE):
                arrive(rates.at[j], ld_s.at[0], ld_r.at[j])
            for n, to in enumerate((above, below, facing)):
                rates_copy(n + 1, to).start()

    lane = lax.broadcasted_iota(jnp.int32, (1, 128), 1)
    low = lax.rem(lane, 64) < 32

    def tables():
        for part in range(SIDE):
            rows = pl.ds(part * ROWS, ROWS)
            at = lax.broadcasted_iota(jnp.int32, (ROWS, 128), 0) + (y * BLOCK + part * ROWS)
            angle = at.astype(F32) * freq_ref[...]
            cosine[rows, :] = jnp.cos(angle)
            turned = jnp.sin(angle)
            sine[rows, :] = jnp.where(low, -turned, turned)

    def decays():
        @pl.when(x != y)
        def _():
            arrive(rates, ld_s.at[0], lr_r.at[0])

        def decay_tiles(h, carry):
            a, b = rates[h, 0:1, :], rates[h, 1:2, :]
            i = lax.broadcasted_iota(jnp.int32, (ROWS, 128), 0)
            j = lax.broadcasted_iota(jnp.int32, (ROWS, 128), 1)
            for m in range(7):
                apart = (i - j + (3 - m) * ROWS).astype(F32)
                rate = jnp.where(apart >= 0.0, a, b)
                value = jnp.exp(rate * jnp.abs(apart))
                tiles[h, :, m * 128:(m + 1) * 128] = jnp.where(apart == 0.0, 2.0, value)
            return carry

        lax.fori_loop(0, OWN, decay_tiles, 0)
        first_head = lane < 64

        def decay_rows(p, carry):
            a = jnp.where(first_head, rates[2 * p, 0:1, :], rates[2 * p + 1, 0:1, :])
            b = jnp.where(first_head, rates[2 * p, 1:2, :], rates[2 * p + 1, 1:2, :])
            t = lax.broadcasted_iota(jnp.int32, (BLOCK, 128), 0).astype(F32)
            decay[p, 0] = jnp.exp((t + 1.0) * a)
            decay[p, 1] = jnp.exp((BLOCK - t) * b)
            decay[p, 2] = jnp.exp((BLOCK - 1.0 - t) * a)
            decay[p, 3] = jnp.exp(t * b)
            return carry

        lax.fori_loop(0, PAIRS, decay_rows, 0)

    def tokens_all():
        arrive(tok.at[left, h1], tok_s.at[2], tok_r.at[2])
        arrive(tok.at[right, h0], tok_s.at[3], tok_r.at[3])
        arrive(tok.at[across, h0], tok_s.at[4], tok_r.at[4])
        arrive(tok.at[across, h1], tok_s.at[5], tok_r.at[5])

    def project(ref, acc, width, offset, fresh):
        at = mod(z + offset, RING)
        rows = tok[:, :, pl.ds(pl.multiple_of(at * 256, 256), 256)].reshape(BLOCK, 256)
        for n in range(width // 256):
            cols = slice(n * 256, (n + 1) * 256)
            part = matmul(rows, ref[pl.ds(at * 2, 2), :, cols].reshape(256, 256))
            acc[:, cols] = part if fresh else acc[:, cols] + part

    def project_many(ref, acc, width, first, count, stride):
        def step(i, carry):
            project(ref, acc, width, first + i * stride, False)
            return carry

        lax.fori_loop(0, count, step, 0)

    def k_project(stage):
        k_or_q(stage, wk, acc_k, KV, wkd_s, wkd_r)

    def q_project(stage):
        k_or_q(stage, wq, acc_q, 256, wqd_s, wqd_r)

    def k_or_q(stage, ref, acc, width, d_s, d_r):
        for n in ((0, 1, 2), (3, 4), (5, 6), (7,))[stage]:
            arrive(ref.at[nth_other(n)], d_s.at[n], d_r.at[n])
        if stage == 0:
            project(ref, acc, width, 0, True)
            project_many(ref, acc, width, 1, 2, 6)
        elif stage == 3:
            project(ref, acc, width, 4, False)
        else:
            project_many(ref, acc, width, stage + 1, 2, 6 - 2 * stage)

    def turn(flat):
        wide = flat.astype(BF16).astype(F32)
        partner = jnp.where(low, pltpu.roll(wide, 96, 1), pltpu.roll(wide, 32, 1))
        return (wide * cosine[...] + partner * sine[...]).astype(BF16)

    row_low = lax.broadcasted_iota(jnp.int32, (128, 1), 0) < 64

    def keys_values():
        for p in range(PAIRS):
            rk = turn(acc_k[:, p * 128:(p + 1) * 128])
            kr[p] = rk
            value = acc_k[:, 256 + p * 256:256 + (p + 1) * 256].astype(BF16)
            vb[2 * p] = value[:, :128]
            vb[2 * p + 1] = value[:, 128:]
            wide_k = rk.astype(F32)
            ks[:, 0:128] = (wide_k * decay[p, 2]).astype(BF16)
            ks[:, 128:256] = (wide_k * decay[p, 3]).astype(BF16)
            both = lax.dot_general(
                ks[...], value, (((0,), (0,)), ((), ())), preferred_element_type=F32
            )
            for d in range(2):
                square = both[d * 128:(d + 1) * 128]
                ab[d, p] = jnp.where(row_low, square[:, :128], square[:, 128:]).astype(BF16)
        for n, to in ((2, facing), (0, above), (1, below)):
            send(ab.at[jnp.where(to > y, 0, 1)], states.at[y], st_s.at[n], st_r.at[n], at_y(to))

    def queries():
        for p in range(PAIRS):
            rq = turn(acc_q[:, p * 128:(p + 1) * 128])
            qr[p] = rq
            wide_q = rq.astype(F32)
            qs[p, :, 0:128] = (wide_q * decay[p, 0]).astype(BF16)
            qs[p, :, 128:256] = (wide_q * decay[p, 1]).astype(BF16)

    def in_block(r):
        rows = pl.ds(pl.multiple_of(r * ROWS, ROWS), ROWS)
        cols = pl.ds(pl.multiple_of((3 - r) * 128, 128), BLOCK)
        for h in range(OWN):
            query = jnp.where((lane >= 64) == (h % 2 == 1), qr[h // 2, rows, :], jnp.zeros((), BF16))
            scores = lax.dot_general(
                query, kr[h // 2], (((1,), (1,)), ((), ())), preferred_element_type=F32
            )
            scores = (scores * tiles[h, :, cols]).astype(BF16)
            ret[r, :, h * 128:(h + 1) * 128] = matmul(scores, vb[h])

    def carry_states():
        arrive(states.at[below], st_s.at[0], st_r.at[0])
        arrive(states.at[above], st_s.at[1], st_r.at[1])
        arrive(states.at[facing], st_s.at[2], st_r.at[2])
        for p in range(PAIRS):
            for d in range(2):
                rate = jnp.where(row_low, rates[2 * p, d:d + 1, 0:1], rates[2 * p + 1, d:d + 1, 0:1])
                total = jnp.zeros((128, 128), F32)
                for o in range(1, SIDE):
                    source = mod(y - o if d == 0 else y + o, SIDE)
                    there = (y - o >= 0) if d == 0 else (y + o < SIDE)
                    weight = jnp.exp(rate * (BLOCK * (o - 1.0)))
                    total = total + jnp.where(there, weight * states[source, p].astype(F32), 0.0)
                total = total.astype(BF16)
                zero = jnp.zeros((), BF16)
                carried[p, d * 128:(d + 1) * 128, 0:128] = jnp.where(row_low, total, zero)
                carried[p, d * 128:(d + 1) * 128, 128:256] = jnp.where(row_low, zero, total)

    def finish_rows(r, dst):
        rows = pl.ds(pl.multiple_of(r * ROWS, ROWS), ROWS)
        for p in range(PAIRS):
            outside = matmul(qs[p, rows, :], carried[p])
            for e in range(2):
                h = 2 * p + e
                whole = ret[r, :, h * 128:(h + 1) * 128] + outside[:, e * 128:(e + 1) * 128]
                centred = whole - jnp.mean(whole, axis=-1, keepdims=True)
                var = jnp.mean(centred * centred, axis=-1, keepdims=True)
                dst[:, h * 128:(h + 1) * 128] = (centred * lax.rsqrt(var + EPS)).astype(BF16)

    to_rows = (across, left, right, x)

    def normed(n):
        r = to_rows[n]
        if n == 3:
            finish_rows(r, nb.at[x])
            return
        finish_rows(r, ns.at[n])
        if n == 0:
            send(ns.at[0, h0], relay.at[0], nb_s.at[0], nb_r.at[0], at_x(right))
            send(ns.at[0, h1], relay.at[1], nb_s.at[1], nb_r.at[1], at_x(left))
        else:
            send(ns.at[n], nb.at[x], nb_s.at[n + 1], nb_r.at[n + 1], at_x(r))

    def normed_forward():
        arrive(relay.at[0], nb_s.at[0], nb_r.at[0])
        send(relay.at[0], nb.at[left, h0], nb_s.at[4], nb_r.at[4], at_x(right))
        arrive(relay.at[1], nb_s.at[1], nb_r.at[1])
        send(relay.at[1], nb.at[right, h1], nb_s.at[5], nb_r.at[5], at_x(left))

    def normed_all():
        arrive(nb.at[right], nb_s.at[2], nb_r.at[2])
        arrive(nb.at[left], nb_s.at[3], nb_r.at[3])
        arrive(nb.at[across, h0], nb_s.at[4], nb_r.at[4])
        arrive(nb.at[across, h1], nb_s.at[5], nb_r.at[5])

    def output(stage):
        if stage == 0:
            normed_all()
        for n in ((0, 1, 2, 3, 4), (5, 6, 7))[stage]:
            take_output(n)
            arrive(wz.at[nth_other(n)], wzd_s.at[n], wzd_r.at[n])
        offsets = ((0, 1, 7, 2, 6), (3, 5, 4))[stage]
        left_hand, blocks = [], []
        for offset in offsets:
            at = mod(z + offset, RING)
            start = pl.multiple_of(lax.rem(at, 2) * 256, 256)
            left_hand.append(nb[lax.div(at, 2), :, pl.ds(start, 256)])
            blocks.append(pl.ds(at * 2, 2))
        for part in range(SIDE + 1):
            width = PART if part < SIDE else REST
            cols = slice(part * PART, part * PART + width)
            total = jnp.zeros((ROWS, width), F32) if stage == 0 else acc_o[:, cols]
            for lhs, rows in zip(left_hand, blocks):
                weight = wo[part, rows] if part < SIDE else wz[rows]
                total = total + matmul(lhs, weight.reshape(256, width))
            if stage == 0:
                acc_o[:, cols] = total
            else:
                out_ref[0, :, cols] = total.astype(BF16)

    def run(name, task, *arguments):
        with jax.named_scope(name):
            for n in needed.get(name, ()):
                fetched[n].wait()
            task(*arguments)

    run("K0", k_step, 0)
    run("LD", send_rates)
    run("T0", tokens_first)
    run("T1", tokens_second)
    run("O0", o_step, 0)
    run("TAB", tables)
    run("K1", k_step, 1)
    run("Q0", q_step, 0)
    run("LF", forward_rates)
    run("TF", tokens_forward)
    run("O1", o_step, 1)
    run("K2", k_step, 2)
    run("Q1", q_step, 1)
    run("O2", o_step, 2)
    run("F1", f_step, 1)
    run("TA", tokens_all)
    run("KA", k_project, 0)
    run("K3", k_step, 3)
    run("QA", q_project, 0)
    run("Q2", q_step, 2)
    run("SO0", own_output_block)
    run("Z0", zz_step, 0)
    run("F2", f_step, 2)
    run("KB", k_project, 1)
    run("D1", d_step, 1)
    run("O3", o_step, 3)
    run("QB", q_project, 1)
    run("G1", g_step, 1)
    run("K4", k_step, 4)
    run("DEC", decays)
    run("D2", d_step, 2)
    run("G2", g_step, 2)
    run("Q3", q_step, 3)
    run("KC", k_project, 2)
    run("KD", k_project, 3)
    run("RK", keys_values)
    run("Z1", zz_step, 1)
    run("O4", o_step, 4)
    run("F3", f_step, 3)
    run("QC", q_project, 2)
    run("Q4", q_step, 4)
    run("QD", q_project, 3)
    run("RQ", queries)
    run("I2", in_block, to_rows[2])
    run("Z2", zz_step, 2)
    run("I0", in_block, to_rows[0])
    run("CAR", carry_states)
    run("N0", normed, 0)
    run("I1", in_block, to_rows[1])
    run("N1", normed, 1)
    run("N2", normed, 2)
    run("F4", f_step, 4)
    run("I3", in_block, to_rows[3])
    run("D4", d_step, 4)
    run("D3", d_step, 3)
    run("Z3", zz_step, 3)
    run("NF", normed_forward)
    run("G3", g_step, 3)
    run("G4", g_step, 4)
    run("Z4", zz_step, 4)
    run("N3", normed, 3)
    run("OA", output, 0)
    run("OB", output, 1)
    for copy in sends:
        copy.wait_send()
    @pl.when(x != y)
    def _():
        rate_copy().wait_send()

    @pl.when(x == y)
    def _():
        for n, to in enumerate((above, below, facing)):
            rates_copy(n + 1, to).wait_send()


def shards(tokens, query_weight, key_weight, value_weight, output_weight, log_decay):
    half_dim = DK // 2
    frequency = (
        np.float32(10000.0) ** (-np.arange(half_dim, dtype=np.float32) / np.float32(half_dim))
    ).astype(np.float32)
    frequency = jnp.asarray(np.tile(frequency, 4)[None, :])
    anywhere = pl.BlockSpec(memory_space=pl.ANY)
    vmem = pl.BlockSpec(memory_space=pltpu.VMEM)
    dma = pltpu.SemaphoreType.DMA
    return pl.pallas_call(
        kernel,
        out_shape=pltpu.VMEM((1, ROWS, D), BF16),
        in_specs=[anywhere] * 7,
        out_specs=vmem,
        scratch_shapes=[
            pltpu.VMEM((SIDE, ROWS, D), BF16),
            pltpu.VMEM((16, 128, 256), BF16),
            pltpu.VMEM((16, 128, KV), BF16),
            pltpu.VMEM((SIDE, 16, 128, PART), BF16),
            pltpu.VMEM((16, 128, REST), BF16),
            pltpu.VMEM((1, 2), F32),
            pltpu.VMEM((1, 128), F32),
            pltpu.VMEM((8, 128), F32),
            pltpu.VMEM((SIDE, 8, 128), F32),
            pltpu.VMEM((BLOCK, 256), F32),
            pltpu.VMEM((BLOCK, KV), F32),
            pltpu.VMEM((BLOCK, 128), F32),
            pltpu.VMEM((BLOCK, 128), F32),
            pltpu.VMEM((OWN, ROWS, 7 * 128), F32),
            pltpu.VMEM((PAIRS, 4, BLOCK, 128), F32),
            pltpu.VMEM((PAIRS, BLOCK, 128), BF16),
            pltpu.VMEM((PAIRS, BLOCK, 128), BF16),
            pltpu.VMEM((OWN, BLOCK, 128), BF16),
            pltpu.VMEM((PAIRS, BLOCK, 256), BF16),
            pltpu.VMEM((BLOCK, 256), BF16),
            pltpu.VMEM((2, PAIRS, 128, 128), BF16),
            pltpu.VMEM((SIDE, PAIRS, 128, 128), BF16),
            pltpu.VMEM((PAIRS, 256, 256), BF16),
            pltpu.VMEM((SIDE, ROWS, 512), F32),
            pltpu.VMEM((3, ROWS, 512), BF16),
            pltpu.VMEM((2, 64, 512), BF16),
            pltpu.VMEM((SIDE, ROWS, 512), BF16),
            pltpu.VMEM((ROWS, D), F32),
            dma((11,)), dma((6,)), dma((6,)),
            dma((2, 4)), dma((2, 4)), dma((8,)), dma((8,)),
            dma((2, 4)), dma((2, 4)), dma((8,)), dma((8,)),
            dma((2, 4)), dma((2, 4)),
            dma((8, 2)), dma((8, 2)), dma((8, 2)), dma((8, 2)),
            dma((8, 4)), dma((8, 4)), dma((1,)), dma((1,)),
            dma((2, 4)), dma((2, 4)), dma((8,)), dma((8,)),
            dma((3,)), dma((3,)), dma((6,)), dma((6,)), dma((4,)), dma((4,)), dma((1,)),
        ],
        compiler_params=pltpu.CompilerParams(
            collective_id=0, has_side_effects=True, vmem_limit_bytes=60 * 1024 * 1024
        ),
        name="retention",
    )(
        tokens, query_weight, key_weight, value_weight, output_weight, log_decay.T, frequency
    )


def solution(mesh):
    placed = (
        P("dp", "sp", None),
        P("dp", None),
        P("dp", None),
        P("dp", None),
        P("dp", None),
        P(None, "sp"),
    )
    return jax.shard_map(
        shards, mesh=mesh, in_specs=placed, out_specs=P("dp", "sp", None), check_vma=False
    )
```

```python
import jax
import jax.numpy as jnp
import numpy as np
from jax import lax
from jax.experimental import pallas as pl
from jax.experimental.pallas import tpu as pltpu
from jax.sharding import PartitionSpec as P

D = 2048
HEADS = 16
DK = 64
DV = 128
BLOCK = 512
ROWS = 128
SIDE = 4
RING = 8
OWN = 4
PAIRS = 2
EPS = 1e-6
KV = 768
PART = 384
REST = 512

F32 = jnp.float32
BF16 = jnp.bfloat16


def mod(value, size):
    return lax.rem(value + size, size)


def matmul(a, b):
    return jnp.dot(a, b, preferred_element_type=F32)


def kernel(
    tok_hbm, q_hbm, k_hbm, v_hbm, o_hbm, ld_hbm, freq_hbm, out_ref,
    tok, wq, wk, wo, wz, ld_ref, freq_ref, own_rate, rates, acc_q, acc_k, cosine, sine, tiles, decay, qr, kr, vb, qs, ks,
    ab, states, carried, ret, ns, relay, nb, acc_o,
    local_sem, tok_s, tok_r, wq_s, wq_r, wqd_s, wqd_r, wk_s, wk_r, wkd_s, wkd_r, wo_s, wo_r,
    wy_s, wy_r, wf_s, wf_r, wod_s, wod_r, wz_s, wz_r, wzd_s, wzd_r, st_s, st_r, nb_s, nb_r, ld_s, ld_r, lr_r,
):
    sp = lax.axis_index("sp")
    dp = lax.axis_index("dp")
    y, x = lax.div(sp, SIDE), lax.rem(sp, SIDE)
    z, c = lax.div(dp, 2), lax.rem(dp, 2)
    right, left, across = mod(x + 1, SIDE), mod(x - 1, SIDE), mod(x + 2, SIDE)
    above, below, facing = mod(y + 1, SIDE), mod(y - 1, SIDE), mod(y + 2, SIDE)
    h0, h1 = pl.ds(0, 64), pl.ds(64, 64)

    def at_x(to):
        return (y * SIDE + to, dp)

    def at_y(to):
        return (to * SIDE + x, dp)

    def at_z(to):
        return (sp, to * 2 + c)

    other_core = (sp, z * 2 + (1 - c))
    def send(src, dst, send_sem, recv_sem, to):
        copy = pltpu.make_async_remote_copy(
            src_ref=src, dst_ref=dst, send_sem=send_sem, recv_sem=recv_sem,
            device_id=to, device_id_type=pl.DeviceIdType.MESH,
        )
        copy.start()

    def arrive(dst, send_sem, recv_sem):
        pltpu.make_async_remote_copy(
            src_ref=dst, dst_ref=dst, send_sem=send_sem, recv_sem=recv_sem,
            device_id=other_core, device_id_type=pl.DeviceIdType.MESH,
        ).wait_recv()

    def fetch(src, dst, n):
        pltpu.make_async_copy(src, dst, local_sem.at[n]).start()

    def fetched(name):
        if name in groups:
            n, ref = groups[name]
            pltpu.make_async_copy(ref, ref, local_sem.at[n]).wait()

    groups = {
        "K0": (0, wk.at[dp]), "T0": (1, tok.at[x]), "LD": (2, ld_ref), "O0": (3, wo.at[:, dp]),
        "Q0": (4, wq.at[dp]), "TAB": (5, freq_ref), "Z0": (6, wz.at[dp]),
    }
    fetch(k_hbm.at[:, pl.ds(pl.multiple_of(x * 256, 256), 256)], wk.at[dp, :, 0:256], 0)
    fetch(v_hbm.at[:, pl.ds(pl.multiple_of(x * 512, 512), 512)], wk.at[dp, :, 256:KV], 0)

    barrier = pltpu.get_barrier_semaphore()
    peers = [at_z(mod(z + 1, RING)), at_z(mod(z - 1, RING)), other_core]
    peers += [at_x(to) for to in (right, left, across)] + [at_y(to) for to in (above, below, facing)]
    for peer in peers:
        pl.semaphore_signal(
            barrier, inc=1, device_id=peer, device_id_type=pl.DeviceIdType.MESH
        )
    fetch(tok_hbm.at[0], tok.at[x], 1)
    fetch(ld_hbm, ld_ref, 2)
    for part in range(SIDE):
        fetch(o_hbm.at[:, part * PART:(part + 1) * PART], wo.at[part, dp], 3)
    fetch(q_hbm.at[:, pl.ds(pl.multiple_of(x * 256, 256), 256)], wq.at[dp], 4)
    fetch(freq_hbm, freq_ref, 5)
    fetch(o_hbm.at[:, SIDE * PART:D], wz.at[dp], 6)
    pl.semaphore_wait(barrier, len(peers))

    def half(direction):
        return h0 if direction == 0 else h1

    def z_block(direction, step):
        return mod(z - step if direction == 0 else z + step, RING) * 2 + c

    def z_next(direction):
        return mod(z + 1 if direction == 0 else z - 1, RING)

    def nth_block(n):
        if n == 0:
            return dp
        if n == 7:
            return z_block(0, 4)
        return z_block((n - 1) % 2, (n + 1) // 2)

    def nth_other(n):
        return nth_block(n) + 1 - 2 * c

    def blocks_of(step):
        return (0,) if step == 0 else (2 * step - 1, 2 * step) if step < 4 else (7,)

    def ring_wait(span, step, s_sem, r_sem):
        if step > 0:
            arrive(span(2 if step < 4 else 1), s_sem.at[0], r_sem.at[step - 1])

    def ring_send(view, step, s_sem, r_sem):
        if step < 4:
            for d in range(2):
                b = z_block(d, step)
                part = view(b) if step < 3 else view(b, half(d))
                send(part, part, s_sem.at[0], r_sem.at[step], at_z(z_next(d)))

    def weight_step(ref, step, s_sem, r_sem, d_s, d_r):
        def view(b, rows=None):
            return ref.at[b] if rows is None else ref.at[b, rows]

        ring_wait(lambda count: ref.at[pl.ds(0, count)], step, s_sem, r_sem)
        ring_send(view, step, s_sem, r_sem)
        for n in blocks_of(step):
            b = nth_block(n)
            group = n // 5 if ref is wz else max(n - 1, 0) // 2
            send(ref.at[b], ref.at[b], d_s.at[0], d_r.at[group], other_core)

    def k_step(step):
        weight_step(wk, step, wk_s, wk_r, wkd_s, wkd_r)

    def q_step(step):
        weight_step(wq, step, wq_s, wq_r, wqd_s, wqd_r)

    def zz_step(step):
        weight_step(wz, step, wz_s, wz_r, wzd_s, wzd_r)

    def share(part, n):
        send(part, part, wod_s.at[0], wod_r.at[n // 5], other_core)

    def o_step(step):
        def view(b, rows=None):
            return wo.at[y, b] if rows is None else wo.at[y, b, rows]

        ring_wait(lambda count: wo.at[0, pl.ds(0, count)], step, wo_s, wo_r)
        ring_send(view, step, wo_s, wo_r)
        if step > 0:
            for n in blocks_of(step):
                part = wo.at[y, nth_block(n)]
                send(part, part, wy_s.at[0], wy_r.at[step - 1], at_y(above))
                send(part, part, wy_s.at[0], wy_r.at[step - 1], at_y(below))

    def f_step(step):
        blocks = blocks_of(step)
        arrive(wo.at[0, pl.ds(0, 2 * len(blocks))], wy_s.at[0], wy_r.at[step - 1])
        for n in blocks:
            b = nth_block(n)
            up, down = wo.at[below, b, h0], wo.at[above, b, h1]
            send(up, up, wf_s.at[0], wf_r.at[step - 1], at_y(above))
            send(down, down, wf_s.at[0], wf_r.at[step - 1], at_y(below))

    def d_step(step):
        for n in blocks_of(step):
            for part in (y, below, above):
                share(wo.at[part, nth_block(n)], n)

    def g_step(step):
        blocks = blocks_of(step)
        arrive(wo.at[0, pl.ds(0, len(blocks))], wf_s.at[0], wf_r.at[step - 1])
        for n in blocks:
            share(wo.at[facing, nth_block(n)], n)

    def own_output_block():
        send(wo.at[:, dp], wo.at[:, dp], wod_s.at[0], wod_r.at[0], other_core)

    def tokens_first():
        send(tok.at[x, h0], tok.at[x, h0], tok_s.at[0], tok_r.at[0], at_x(right))
        send(tok.at[x, h1], tok.at[x, h1], tok_s.at[0], tok_r.at[0], at_x(left))

    def tokens_second():
        send(tok.at[x, h1], tok.at[x, h1], tok_s.at[0], tok_r.at[1], at_x(right))
        send(tok.at[x, h0], tok.at[x, h0], tok_s.at[0], tok_r.at[1], at_x(left))

    def tokens_forward():
        arrive(tok.at[0], tok_s.at[0], tok_r.at[0])
        send(tok.at[left, h0], tok.at[left, h0], tok_s.at[0], tok_r.at[1], at_x(right))
        send(tok.at[right, h1], tok.at[right, h1], tok_s.at[0], tok_r.at[1], at_x(left))

    def rate_copy():
        return pltpu.make_async_remote_copy(
            src_ref=own_rate, dst_ref=rates.at[x], send_sem=ld_s.at[0], recv_sem=ld_r.at[0],
            device_id=at_x(y), device_id_type=pl.DeviceIdType.MESH,
        )

    def rates_copy(n, to):
        return pltpu.make_async_remote_copy(
            src_ref=rates, dst_ref=rates, send_sem=ld_s.at[n], recv_sem=lr_r.at[0],
            device_id=at_y(to), device_id_type=pl.DeviceIdType.MESH,
        )

    def send_rates():
        sub = lax.broadcasted_iota(jnp.int32, (8, 128), 0)
        own_rate[...] = jnp.where(sub == 0, ld_ref[0:1, 0:1], ld_ref[0:1, 1:2])

        @pl.when(x != y)
        def _():
            rate_copy().start()

        @pl.when(x == y)
        def _():
            pltpu.make_async_copy(own_rate, rates.at[x], ld_r.at[0]).start()

    def forward_rates():
        @pl.when(x == y)
        def _():
            arrive(rates, ld_s.at[0], ld_r.at[0])
            for n, to in enumerate((above, below, facing)):
                rates_copy(n + 1, to).start()

    lane = lax.broadcasted_iota(jnp.int32, (1, 128), 1)
    low = lax.rem(lane, 64) < 32

    def tables():
        for part in range(SIDE):
            rows = pl.ds(part * ROWS, ROWS)
            at = lax.broadcasted_iota(jnp.int32, (ROWS, 128), 0) + (y * BLOCK + part * ROWS)
            angle = at.astype(F32) * freq_ref[...]
            cosine[rows, :] = jnp.cos(angle)
            turned = jnp.sin(angle)
            sine[rows, :] = jnp.where(low, -turned, turned)

    def decays():
        @pl.when(x != y)
        def _():
            arrive(rates, ld_s.at[0], lr_r.at[0])

        def decay_tiles(h, carry):
            a, b = rates[h, 0:1, :], rates[h, 1:2, :]
            i = lax.broadcasted_iota(jnp.int32, (ROWS, 128), 0)
            j = lax.broadcasted_iota(jnp.int32, (ROWS, 128), 1)
            for m in range(7):
                apart = (i - j + (3 - m) * ROWS).astype(F32)
                rate = jnp.where(apart >= 0.0, a, b)
                value = jnp.exp(rate * jnp.abs(apart))
                tiles[h, :, m * 128:(m + 1) * 128] = jnp.where(apart == 0.0, 2.0, value)
            return carry

        lax.fori_loop(0, OWN, decay_tiles, 0)
        first_head = lane < 64

        def decay_rows(p, carry):
            a = jnp.where(first_head, rates[2 * p, 0:1, :], rates[2 * p + 1, 0:1, :])
            b = jnp.where(first_head, rates[2 * p, 1:2, :], rates[2 * p + 1, 1:2, :])
            t = lax.broadcasted_iota(jnp.int32, (BLOCK, 128), 0).astype(F32)
            decay[p, 0] = jnp.exp((t + 1.0) * a)
            decay[p, 1] = jnp.exp((BLOCK - t) * b)
            decay[p, 2] = jnp.exp((BLOCK - 1.0 - t) * a)
            decay[p, 3] = jnp.exp(t * b)
            return carry

        lax.fori_loop(0, PAIRS, decay_rows, 0)

    def tokens_all():
        arrive(tok.at[pl.ds(0, 2)], tok_s.at[0], tok_r.at[1])

    def project(ref, acc, width, offset, fresh):
        at = mod(z + offset, RING)
        rows = tok[:, :, pl.ds(pl.multiple_of(at * 256, 256), 256)].reshape(BLOCK, 256)
        for n in range(width // 256):
            cols = slice(n * 256, (n + 1) * 256)
            part = matmul(rows, ref[pl.ds(at * 2, 2), :, cols].reshape(256, 256))
            acc[:, cols] = part if fresh else acc[:, cols] + part

    def project_many(ref, acc, width, first, count, stride):
        def step(i, carry):
            project(ref, acc, width, first + i * stride, False)
            return carry

        lax.fori_loop(0, count, step, 0)

    def k_project(stage):
        k_or_q(stage, wk, acc_k, KV, wkd_s, wkd_r)

    def q_project(stage):
        k_or_q(stage, wq, acc_q, 256, wqd_s, wqd_r)

    def k_or_q(stage, ref, acc, width, d_s, d_r):
        arrive(ref.at[pl.ds(0, (3, 2, 2, 1)[stage])], d_s.at[0], d_r.at[stage])
        if stage == 0:
            project(ref, acc, width, 0, True)
            project_many(ref, acc, width, 1, 2, 6)
        elif stage == 3:
            project(ref, acc, width, 4, False)
        else:
            project_many(ref, acc, width, stage + 1, 2, 6 - 2 * stage)

    def turn(flat):
        wide = flat.astype(BF16).astype(F32)
        partner = jnp.where(low, pltpu.roll(wide, 96, 1), pltpu.roll(wide, 32, 1))
        return (wide * cosine[...] + partner * sine[...]).astype(BF16)

    row_low = lax.broadcasted_iota(jnp.int32, (128, 1), 0) < 64

    def keys_values():
        for p in range(PAIRS):
            rk = turn(acc_k[:, p * 128:(p + 1) * 128])
            kr[p] = rk
            value = acc_k[:, 256 + p * 256:256 + (p + 1) * 256].astype(BF16)
            vb[2 * p] = value[:, :128]
            vb[2 * p + 1] = value[:, 128:]
            wide_k = rk.astype(F32)
            ks[:, 0:128] = (wide_k * decay[p, 2]).astype(BF16)
            ks[:, 128:256] = (wide_k * decay[p, 3]).astype(BF16)
            both = lax.dot_general(
                ks[...], value, (((0,), (0,)), ((), ())), preferred_element_type=F32
            )
            for d in range(2):
                square = both[d * 128:(d + 1) * 128]
                ab[d, p] = jnp.where(row_low, square[:, :128], square[:, 128:]).astype(BF16)
        for to in (facing, above, below):
            send(ab.at[jnp.where(to > y, 0, 1)], states.at[y], st_s.at[0], st_r.at[0], at_y(to))

    def queries():
        for p in range(PAIRS):
            rq = turn(acc_q[:, p * 128:(p + 1) * 128])
            qr[p] = rq
            wide_q = rq.astype(F32)
            qs[p, :, 0:128] = (wide_q * decay[p, 0]).astype(BF16)
            qs[p, :, 128:256] = (wide_q * decay[p, 1]).astype(BF16)

    def in_block(r):
        rows = pl.ds(pl.multiple_of(r * ROWS, ROWS), ROWS)
        cols = pl.ds(pl.multiple_of((3 - r) * 128, 128), BLOCK)
        for h in range(OWN):
            query = jnp.where((lane >= 64) == (h % 2 == 1), qr[h // 2, rows, :], jnp.zeros((), BF16))
            scores = lax.dot_general(
                query, kr[h // 2], (((1,), (1,)), ((), ())), preferred_element_type=F32
            )
            scores = (scores * tiles[h, :, cols]).astype(BF16)
            ret[r, :, h * 128:(h + 1) * 128] = matmul(scores, vb[h])

    def carry_states():
        arrive(states.at[pl.ds(0, 3)], st_s.at[0], st_r.at[0])
        for p in range(PAIRS):
            for d in range(2):
                rate = jnp.where(row_low, rates[2 * p, d:d + 1, 0:1], rates[2 * p + 1, d:d + 1, 0:1])
                total = jnp.zeros((128, 128), F32)
                for o in range(1, SIDE):
                    source = mod(y - o if d == 0 else y + o, SIDE)
                    there = (y - o >= 0) if d == 0 else (y + o < SIDE)
                    weight = jnp.exp(rate * (BLOCK * (o - 1.0)))
                    total = total + jnp.where(there, weight * states[source, p].astype(F32), 0.0)
                total = total.astype(BF16)
                zero = jnp.zeros((), BF16)
                carried[p, d * 128:(d + 1) * 128, 0:128] = jnp.where(row_low, total, zero)
                carried[p, d * 128:(d + 1) * 128, 128:256] = jnp.where(row_low, zero, total)

    def finish_rows(r, dst):
        rows = pl.ds(pl.multiple_of(r * ROWS, ROWS), ROWS)
        for p in range(PAIRS):
            outside = matmul(qs[p, rows, :], carried[p])
            for e in range(2):
                h = 2 * p + e
                whole = ret[r, :, h * 128:(h + 1) * 128] + outside[:, e * 128:(e + 1) * 128]
                centred = whole - jnp.mean(whole, axis=-1, keepdims=True)
                var = jnp.mean(centred * centred, axis=-1, keepdims=True)
                dst[:, h * 128:(h + 1) * 128] = (centred * lax.rsqrt(var + EPS)).astype(BF16)

    to_rows = (across, left, right, x)

    def normed(n):
        r = to_rows[n]
        if n == 3:
            finish_rows(r, nb.at[x])
            return
        finish_rows(r, ns.at[n])
        if n == 0:
            send(ns.at[0, h0], relay.at[0], nb_s.at[0], nb_r.at[0], at_x(right))
            send(ns.at[0, h1], relay.at[1], nb_s.at[0], nb_r.at[0], at_x(left))
        else:
            send(ns.at[n], nb.at[x], nb_s.at[0], nb_r.at[1], at_x(r))

    def normed_forward():
        arrive(relay, nb_s.at[0], nb_r.at[0])
        send(relay.at[0], nb.at[left, h0], nb_s.at[0], nb_r.at[1], at_x(right))
        send(relay.at[1], nb.at[right, h1], nb_s.at[0], nb_r.at[1], at_x(left))

    def normed_all():
        arrive(nb.at[pl.ds(0, 3)], nb_s.at[0], nb_r.at[1])

    def output(stage):
        if stage == 0:
            normed_all()
        count = (5, 3)[stage]
        arrive(wo.at[:, pl.ds(0, count)], wod_s.at[0], wod_r.at[stage])
        arrive(wz.at[pl.ds(0, count)], wzd_s.at[0], wzd_r.at[stage])
        offsets = ((0, 1, 7, 2, 6), (3, 5, 4))[stage]
        left_hand, blocks = [], []
        for offset in offsets:
            at = mod(z + offset, RING)
            start = pl.multiple_of(lax.rem(at, 2) * 256, 256)
            left_hand.append(nb[lax.div(at, 2), :, pl.ds(start, 256)])
            blocks.append(pl.ds(at * 2, 2))
        for part in range(SIDE + 1):
            width = PART if part < SIDE else REST
            cols = slice(part * PART, part * PART + width)
            total = jnp.zeros((ROWS, width), F32) if stage == 0 else acc_o[:, cols]
            for lhs, rows in zip(left_hand, blocks):
                weight = wo[part, rows] if part < SIDE else wz[rows]
                total = total + matmul(lhs, weight.reshape(256, width))
            if stage == 0:
                acc_o[:, cols] = total
            else:
                out_ref[0, :, cols] = total.astype(BF16)

    def run(name, task, *arguments):
        with jax.named_scope(name):
            fetched(name)
            task(*arguments)

    run("K0", k_step, 0)
    run("LD", send_rates)
    run("T0", tokens_first)
    run("T1", tokens_second)
    run("O0", o_step, 0)
    run("TAB", tables)
    run("K1", k_step, 1)
    run("Q0", q_step, 0)
    run("LF", forward_rates)
    run("TF", tokens_forward)
    run("O1", o_step, 1)
    run("K2", k_step, 2)
    run("Q1", q_step, 1)
    run("O2", o_step, 2)
    run("F1", f_step, 1)
    run("TA", tokens_all)
    run("KA", k_project, 0)
    run("K3", k_step, 3)
    run("QA", q_project, 0)
    run("Q2", q_step, 2)
    run("SO0", own_output_block)
    run("Z0", zz_step, 0)
    run("F2", f_step, 2)
    run("KB", k_project, 1)
    run("D1", d_step, 1)
    run("O3", o_step, 3)
    run("QB", q_project, 1)
    run("G1", g_step, 1)
    run("K4", k_step, 4)
    run("DEC", decays)
    run("D2", d_step, 2)
    run("G2", g_step, 2)
    run("Q3", q_step, 3)
    run("KC", k_project, 2)
    run("KD", k_project, 3)
    run("RK", keys_values)
    run("Z1", zz_step, 1)
    run("O4", o_step, 4)
    run("F3", f_step, 3)
    run("QC", q_project, 2)
    run("Q4", q_step, 4)
    run("QD", q_project, 3)
    run("RQ", queries)
    run("I2", in_block, to_rows[2])
    run("Z2", zz_step, 2)
    run("I0", in_block, to_rows[0])
    run("CAR", carry_states)
    run("N0", normed, 0)
    run("I1", in_block, to_rows[1])
    run("N1", normed, 1)
    run("N2", normed, 2)
    run("F4", f_step, 4)
    run("I3", in_block, to_rows[3])
    run("D4", d_step, 4)
    run("D3", d_step, 3)
    run("Z3", zz_step, 3)
    run("NF", normed_forward)
    run("G3", g_step, 3)
    run("G4", g_step, 4)
    run("Z4", zz_step, 4)
    run("N3", normed, 3)
    run("OA", output, 0)
    run("OB", output, 1)
    for ref, sem in (
        (tok.at[pl.ds(0, 3)], tok_s), (wq.at[pl.ds(0, 7)], wq_s), (wk.at[pl.ds(0, 7)], wk_s),
        (wz.at[pl.ds(0, 7)], wz_s), (wo.at[0, pl.ds(0, 7)], wo_s), (wq.at[pl.ds(0, 8)], wqd_s),
        (wk.at[pl.ds(0, 8)], wkd_s), (wz.at[pl.ds(0, 8)], wzd_s), (wo.at[:, pl.ds(0, 8)], wod_s),
        (wo.at[0, pl.ds(0, 14)], wy_s), (wo.at[0, pl.ds(0, 7)], wf_s),
        (states.at[pl.ds(0, 3)], st_s), (nb, nb_s),
    ):
        pltpu.make_async_remote_copy(
            src_ref=ref, dst_ref=ref, send_sem=sem.at[0], recv_sem=lr_r.at[0],
            device_id=other_core, device_id_type=pl.DeviceIdType.MESH,
        ).wait_send()
    @pl.when(x != y)
    def _():
        rate_copy().wait_send()

    @pl.when(x == y)
    def _():
        for n, to in enumerate((above, below, facing)):
            rates_copy(n + 1, to).wait_send()


def shards(tokens, query_weight, key_weight, value_weight, output_weight, log_decay):
    half_dim = DK // 2
    frequency = (
        np.float32(10000.0) ** (-np.arange(half_dim, dtype=np.float32) / np.float32(half_dim))
    ).astype(np.float32)
    frequency = jnp.asarray(np.tile(frequency, 4)[None, :])
    anywhere = pl.BlockSpec(memory_space=pl.ANY)
    vmem = pl.BlockSpec(memory_space=pltpu.VMEM)
    dma = pltpu.SemaphoreType.DMA
    return pl.pallas_call(
        kernel,
        out_shape=pltpu.VMEM((1, ROWS, D), BF16),
        in_specs=[anywhere] * 7,
        out_specs=vmem,
        scratch_shapes=[
            pltpu.VMEM((SIDE, ROWS, D), BF16),
            pltpu.VMEM((16, 128, 256), BF16),
            pltpu.VMEM((16, 128, KV), BF16),
            pltpu.VMEM((SIDE, 16, 128, PART), BF16),
            pltpu.VMEM((16, 128, REST), BF16),
            pltpu.VMEM((1, 2), F32),
            pltpu.VMEM((1, 128), F32),
            pltpu.VMEM((8, 128), F32),
            pltpu.VMEM((SIDE, 8, 128), F32),
            pltpu.VMEM((BLOCK, 256), F32),
            pltpu.VMEM((BLOCK, KV), F32),
            pltpu.VMEM((BLOCK, 128), F32),
            pltpu.VMEM((BLOCK, 128), F32),
            pltpu.VMEM((OWN, ROWS, 7 * 128), F32),
            pltpu.VMEM((PAIRS, 4, BLOCK, 128), F32),
            pltpu.VMEM((PAIRS, BLOCK, 128), BF16),
            pltpu.VMEM((PAIRS, BLOCK, 128), BF16),
            pltpu.VMEM((OWN, BLOCK, 128), BF16),
            pltpu.VMEM((PAIRS, BLOCK, 256), BF16),
            pltpu.VMEM((BLOCK, 256), BF16),
            pltpu.VMEM((2, PAIRS, 128, 128), BF16),
            pltpu.VMEM((SIDE, PAIRS, 128, 128), BF16),
            pltpu.VMEM((PAIRS, 256, 256), BF16),
            pltpu.VMEM((SIDE, ROWS, 512), F32),
            pltpu.VMEM((3, ROWS, 512), BF16),
            pltpu.VMEM((2, 64, 512), BF16),
            pltpu.VMEM((SIDE, ROWS, 512), BF16),
            pltpu.VMEM((ROWS, D), F32),
            dma((7,)), dma((1,)), dma((2,)),
            dma((1,)), dma((4,)), dma((1,)), dma((4,)),
            dma((1,)), dma((4,)), dma((1,)), dma((4,)),
            dma((1,)), dma((4,)),
            dma((1,)), dma((4,)), dma((1,)), dma((4,)),
            dma((1,)), dma((2,)),
            dma((1,)), dma((4,)), dma((1,)), dma((2,)),
            dma((1,)), dma((1,)), dma((1,)), dma((2,)), dma((4,)), dma((1,)), dma((1,)),
        ],
        compiler_params=pltpu.CompilerParams(
            collective_id=0, has_side_effects=True, vmem_limit_bytes=60 * 1024 * 1024
        ),
        name="retention",
    )(
        tokens, query_weight, key_weight, value_weight, output_weight, log_decay.T, frequency
    )


def solution(mesh):
    placed = (
        P("dp", "sp", None),
        P("dp", None),
        P("dp", None),
        P("dp", None),
        P("dp", None),
        P(None, "sp"),
    )
    return jax.shard_map(
        shards, mesh=mesh, in_specs=placed, out_specs=P("dp", "sp", None), check_vma=False
    )
```

```python
import jax
import jax.numpy as jnp
import numpy as np
from jax import lax
from jax.experimental import pallas as pl
from jax.experimental.pallas import tpu as pltpu
from jax.sharding import PartitionSpec as P

D = 2048
HEADS = 16
DK = 64
DV = 128
BLOCK = 512
ROWS = 128
SIDE = 4
RING = 8
OWN = 4
PAIRS = 2
EPS = 1e-6
KV = 768
PART = 384
REST = 512

F32 = jnp.float32
BF16 = jnp.bfloat16


def mod(value, size):
    return lax.rem(value + size, size)


def matmul(a, b):
    return jnp.dot(a, b, preferred_element_type=F32)


def kernel(
    tok_hbm, q_hbm, k_hbm, v_hbm, o_hbm, ld_hbm, freq_hbm, out_ref,
    tok, wq, wk, wo, wz, ld_ref, freq_ref, own_rate, rates, acc_q, acc_k, cosine, sine, tiles, decay, qr, kr, vb, qs, ks,
    ab, states, carried, ret, ns, relay, nb, acc_o,
    local_sem, tok_s, tok_r, wq_s, wq_r, wqd_s, wqd_r, wk_s, wk_r, wkd_s, wkd_r, wo_s, wo_r,
    wy_s, wy_r, wf_s, wf_r, wod_s, wod_r, wz_s, wz_r, wzd_s, wzd_r, st_s, st_r, nb_s, nb_r, ld_s, ld_r, lr_r,
):
    sp = lax.axis_index("sp")
    dp = lax.axis_index("dp")
    y, x = lax.div(sp, SIDE), lax.rem(sp, SIDE)
    z, c = lax.div(dp, 2), lax.rem(dp, 2)
    right, left, across = mod(x + 1, SIDE), mod(x - 1, SIDE), mod(x + 2, SIDE)
    above, below, facing = mod(y + 1, SIDE), mod(y - 1, SIDE), mod(y + 2, SIDE)
    h0, h1 = pl.ds(0, 64), pl.ds(64, 64)

    def at_x(to):
        return (y * SIDE + to, dp)

    def at_y(to):
        return (to * SIDE + x, dp)

    def at_z(to):
        return (sp, to * 2 + c)

    other_core = (sp, z * 2 + (1 - c))
    def send(src, dst, send_sem, recv_sem, to):
        copy = pltpu.make_async_remote_copy(
            src_ref=src, dst_ref=dst, send_sem=send_sem, recv_sem=recv_sem,
            device_id=to, device_id_type=pl.DeviceIdType.MESH,
        )
        copy.start()

    def arrive(dst, send_sem, recv_sem):
        pltpu.make_async_remote_copy(
            src_ref=dst, dst_ref=dst, send_sem=send_sem, recv_sem=recv_sem,
            device_id=other_core, device_id_type=pl.DeviceIdType.MESH,
        ).wait_recv()

    def fetch(src, dst, n):
        pltpu.make_async_copy(src, dst, local_sem.at[n]).start()

    def fetched(name):
        if name in groups:
            n, ref = groups[name]
            pltpu.make_async_copy(ref, ref, local_sem.at[n]).wait()

    groups = {
        "K0": (0, wk.at[dp]), "T0": (1, tok.at[x]), "LD": (2, ld_ref), "O0": (3, wo.at[:, dp]),
        "Q0": (4, wq.at[dp]), "TAB": (5, freq_ref), "Z0": (6, wz.at[dp]),
    }
    fetch(k_hbm.at[:, pl.ds(pl.multiple_of(x * 256, 256), 256)], wk.at[dp, :, 0:256], 0)
    fetch(v_hbm.at[:, pl.ds(pl.multiple_of(x * 512, 512), 512)], wk.at[dp, :, 256:KV], 0)

    barrier = pltpu.get_barrier_semaphore()
    peers = [at_z(mod(z + 1, RING)), at_z(mod(z - 1, RING)), other_core]
    peers += [at_x(to) for to in (right, left, across)] + [at_y(to) for to in (above, below, facing)]
    for peer in peers:
        pl.semaphore_signal(
            barrier, inc=1, device_id=peer, device_id_type=pl.DeviceIdType.MESH
        )
    fetch(tok_hbm.at[0], tok.at[x], 1)
    fetch(ld_hbm, ld_ref, 2)
    for part in range(SIDE):
        fetch(o_hbm.at[:, part * PART:(part + 1) * PART], wo.at[part, dp], 3)
    fetch(q_hbm.at[:, pl.ds(pl.multiple_of(x * 256, 256), 256)], wq.at[dp], 4)
    fetch(freq_hbm, freq_ref, 5)
    fetch(o_hbm.at[:, SIDE * PART:D], wz.at[dp], 6)
    pl.semaphore_wait(barrier, len(peers))

    def half(direction):
        return h0 if direction == 0 else h1

    def z_block(direction, step):
        return mod(z - step if direction == 0 else z + step, RING) * 2 + c

    def z_next(direction):
        return mod(z + 1 if direction == 0 else z - 1, RING)

    def nth_block(n):
        if n == 0:
            return dp
        if n == 7:
            return z_block(0, 4)
        return z_block((n - 1) % 2, (n + 1) // 2)

    def nth_other(n):
        return nth_block(n) + 1 - 2 * c

    def blocks_of(step):
        return (0,) if step == 0 else (2 * step - 1, 2 * step) if step < 4 else (7,)

    def ring_wait(span, step, s_sem, r_sem):
        if step > 0:
            arrive(span(2 if step < 4 else 1), s_sem.at[0], r_sem.at[step - 1])

    def ring_send(view, step, s_sem, r_sem):
        if step < 4:
            for d in range(2):
                b = z_block(d, step)
                part = view(b) if step < 3 else view(b, half(d))
                send(part, part, s_sem.at[0], r_sem.at[step], at_z(z_next(d)))

    def weight_step(ref, step, s_sem, r_sem, d_s, d_r):
        def view(b, rows=None):
            return ref.at[b] if rows is None else ref.at[b, rows]

        ring_wait(lambda count: ref.at[pl.ds(0, count)], step, s_sem, r_sem)
        ring_send(view, step, s_sem, r_sem)
        for n in blocks_of(step):
            b = nth_block(n)
            group = n // 5 if ref is wz else max(n - 1, 0) // 2
            send(ref.at[b], ref.at[b], d_s.at[0], d_r.at[group], other_core)

    def k_step(step):
        weight_step(wk, step, wk_s, wk_r, wkd_s, wkd_r)

    def q_step(step):
        weight_step(wq, step, wq_s, wq_r, wqd_s, wqd_r)

    def zz_step(step):
        weight_step(wz, step, wz_s, wz_r, wzd_s, wzd_r)

    def share(part, n):
        send(part, part, wod_s.at[0], wod_r.at[n // 5], other_core)

    def o_step(step):
        def view(b, rows=None):
            return wo.at[y, b] if rows is None else wo.at[y, b, rows]

        ring_wait(lambda count: wo.at[0, pl.ds(0, count)], step, wo_s, wo_r)
        ring_send(view, step, wo_s, wo_r)
        if step > 0:
            for n in blocks_of(step):
                part = wo.at[y, nth_block(n)]
                send(part, part, wy_s.at[0], wy_r.at[step - 1], at_y(above))
                send(part, part, wy_s.at[0], wy_r.at[step - 1], at_y(below))

    def f_step(step):
        blocks = blocks_of(step)
        arrive(wo.at[0, pl.ds(0, 2 * len(blocks))], wy_s.at[0], wy_r.at[step - 1])
        for n in blocks:
            b = nth_block(n)
            up, down = wo.at[below, b, h0], wo.at[above, b, h1]
            send(up, up, wf_s.at[0], wf_r.at[step - 1], at_y(above))
            send(down, down, wf_s.at[0], wf_r.at[step - 1], at_y(below))

    def d_step(step):
        for n in blocks_of(step):
            for part in (y, below, above):
                share(wo.at[part, nth_block(n)], n)

    def g_step(step):
        blocks = blocks_of(step)
        arrive(wo.at[0, pl.ds(0, len(blocks))], wf_s.at[0], wf_r.at[step - 1])
        for n in blocks:
            share(wo.at[facing, nth_block(n)], n)

    def own_output_block():
        send(wo.at[:, dp], wo.at[:, dp], wod_s.at[0], wod_r.at[0], other_core)

    def tokens_first():
        send(tok.at[x, h0], tok.at[x, h0], tok_s.at[0], tok_r.at[0], at_x(right))
        send(tok.at[x, h1], tok.at[x, h1], tok_s.at[0], tok_r.at[0], at_x(left))

    def tokens_second():
        send(tok.at[x, h1], tok.at[x, h1], tok_s.at[0], tok_r.at[1], at_x(right))
        send(tok.at[x, h0], tok.at[x, h0], tok_s.at[0], tok_r.at[1], at_x(left))

    def tokens_forward():
        arrive(tok.at[0], tok_s.at[0], tok_r.at[0])
        send(tok.at[left, h0], tok.at[left, h0], tok_s.at[0], tok_r.at[1], at_x(right))
        send(tok.at[right, h1], tok.at[right, h1], tok_s.at[0], tok_r.at[1], at_x(left))

    def rate_copy():
        return pltpu.make_async_remote_copy(
            src_ref=own_rate, dst_ref=rates.at[x], send_sem=ld_s.at[0], recv_sem=ld_r.at[0],
            device_id=at_x(y), device_id_type=pl.DeviceIdType.MESH,
        )

    def rates_copy(n, to):
        return pltpu.make_async_remote_copy(
            src_ref=rates, dst_ref=rates, send_sem=ld_s.at[n], recv_sem=lr_r.at[0],
            device_id=at_y(to), device_id_type=pl.DeviceIdType.MESH,
        )

    def send_rates():
        sub = lax.broadcasted_iota(jnp.int32, (8, 128), 0)
        own_rate[...] = jnp.where(sub == 0, ld_ref[0:1, 0:1], ld_ref[0:1, 1:2])

        @pl.when(x != y)
        def _():
            rate_copy().start()

        @pl.when(x == y)
        def _():
            pltpu.make_async_copy(own_rate, rates.at[x], ld_r.at[0]).start()

    def forward_rates():
        @pl.when(x == y)
        def _():
            arrive(rates, ld_s.at[0], ld_r.at[0])
            for n, to in enumerate((above, below, facing)):
                rates_copy(n + 1, to).start()

    lane = lax.broadcasted_iota(jnp.int32, (1, 128), 1)
    low = lax.rem(lane, 64) < 32

    def tables():
        for part in range(SIDE):
            rows = pl.ds(part * ROWS, ROWS)
            at = lax.broadcasted_iota(jnp.int32, (ROWS, 128), 0) + (y * BLOCK + part * ROWS)
            angle = at.astype(F32) * freq_ref[...]
            cosine[rows, :] = jnp.cos(angle)
            turned = jnp.sin(angle)
            sine[rows, :] = jnp.where(low, -turned, turned)

    def decays():
        @pl.when(x != y)
        def _():
            arrive(rates, ld_s.at[0], lr_r.at[0])

        def decay_tiles(h, carry):
            a, b = rates[h, 0:1, :], rates[h, 1:2, :]
            i = lax.broadcasted_iota(jnp.int32, (ROWS, 128), 0)
            j = lax.broadcasted_iota(jnp.int32, (ROWS, 128), 1)
            for m in range(7):
                apart = (i - j + (3 - m) * ROWS).astype(F32)
                rate = jnp.where(apart >= 0.0, a, b)
                value = jnp.exp(rate * jnp.abs(apart))
                tiles[h, :, m * 128:(m + 1) * 128] = jnp.where(apart == 0.0, 2.0, value)
            return carry

        lax.fori_loop(0, OWN, decay_tiles, 0)
        first_head = lane < 64

        def decay_rows(p, carry):
            a = jnp.where(first_head, rates[2 * p, 0:1, :], rates[2 * p + 1, 0:1, :])
            b = jnp.where(first_head, rates[2 * p, 1:2, :], rates[2 * p + 1, 1:2, :])
            t = lax.broadcasted_iota(jnp.int32, (BLOCK, 128), 0).astype(F32)
            decay[p, 0] = jnp.exp((t + 1.0) * a)
            decay[p, 1] = jnp.exp((BLOCK - t) * b)
            decay[p, 2] = jnp.exp((BLOCK - 1.0 - t) * a)
            decay[p, 3] = jnp.exp(t * b)
            return carry

        lax.fori_loop(0, PAIRS, decay_rows, 0)

    def tokens_all():
        arrive(tok.at[pl.ds(0, 2)], tok_s.at[0], tok_r.at[1])

    def project(ref, acc, width, offset, fresh):
        at = mod(z + offset, RING)
        rows = tok[:, :, pl.ds(pl.multiple_of(at * 256, 256), 256)].reshape(BLOCK, 256)
        for n in range(width // 256):
            cols = slice(n * 256, (n + 1) * 256)
            part = matmul(rows, ref[pl.ds(at * 2, 2), :, cols].reshape(256, 256))
            acc[:, cols] = part if fresh else acc[:, cols] + part

    def project_many(ref, acc, width, first, count, stride):
        def step(i, carry):
            project(ref, acc, width, first + i * stride, False)
            return carry

        lax.fori_loop(0, count, step, 0)

    def k_project(stage):
        k_or_q(stage, wk, acc_k, KV, wkd_s, wkd_r)

    def q_project(stage):
        k_or_q(stage, wq, acc_q, 256, wqd_s, wqd_r)

    def k_or_q(stage, ref, acc, width, d_s, d_r):
        arrive(ref.at[pl.ds(0, (3, 2, 2, 1)[stage])], d_s.at[0], d_r.at[stage])
        if stage == 0:
            project(ref, acc, width, 0, True)
            project_many(ref, acc, width, 1, 2, 6)
        elif stage == 3:
            project(ref, acc, width, 4, False)
        else:
            project_many(ref, acc, width, stage + 1, 2, 6 - 2 * stage)

    def turn(flat):
        wide = flat.astype(BF16).astype(F32)
        partner = jnp.where(low, pltpu.roll(wide, 96, 1), pltpu.roll(wide, 32, 1))
        return (wide * cosine[...] + partner * sine[...]).astype(BF16)

    row_low = lax.broadcasted_iota(jnp.int32, (128, 1), 0) < 64

    def keys_values():
        for p in range(PAIRS):
            rk = turn(acc_k[:, p * 128:(p + 1) * 128])
            kr[p] = rk
            value = acc_k[:, 256 + p * 256:256 + (p + 1) * 256].astype(BF16)
            vb[2 * p] = value[:, :128]
            vb[2 * p + 1] = value[:, 128:]
            wide_k = rk.astype(F32)
            ks[:, 0:128] = (wide_k * decay[p, 2]).astype(BF16)
            ks[:, 128:256] = (wide_k * decay[p, 3]).astype(BF16)
            both = lax.dot_general(
                ks[...], value, (((0,), (0,)), ((), ())), preferred_element_type=F32
            )
            for d in range(2):
                square = both[d * 128:(d + 1) * 128]
                ab[d, p] = jnp.where(row_low, square[:, :128], square[:, 128:]).astype(BF16)
        for to in (facing, above, below):
            send(ab.at[jnp.where(to > y, 0, 1)], states.at[y], st_s.at[0], st_r.at[0], at_y(to))

    def queries():
        for p in range(PAIRS):
            rq = turn(acc_q[:, p * 128:(p + 1) * 128])
            qr[p] = rq
            wide_q = rq.astype(F32)
            qs[p, :, 0:128] = (wide_q * decay[p, 0]).astype(BF16)
            qs[p, :, 128:256] = (wide_q * decay[p, 1]).astype(BF16)

    def in_block(r):
        rows = pl.ds(pl.multiple_of(r * ROWS, ROWS), ROWS)
        cols = pl.ds(pl.multiple_of((3 - r) * 128, 128), BLOCK)
        for h in range(OWN):
            query = jnp.where((lane >= 64) == (h % 2 == 1), qr[h // 2, rows, :], jnp.zeros((), BF16))
            scores = lax.dot_general(
                query, kr[h // 2], (((1,), (1,)), ((), ())), preferred_element_type=F32
            )
            scores = (scores * tiles[h, :, cols]).astype(BF16)
            ret[r, :, h * 128:(h + 1) * 128] = matmul(scores, vb[h])

    def carry_states():
        arrive(states.at[pl.ds(0, 3)], st_s.at[0], st_r.at[0])
        for p in range(PAIRS):
            for d in range(2):
                rate = jnp.where(row_low, rates[2 * p, d:d + 1, 0:1], rates[2 * p + 1, d:d + 1, 0:1])
                total = jnp.zeros((128, 128), F32)
                for o in range(1, SIDE):
                    source = mod(y - o if d == 0 else y + o, SIDE)
                    there = (y - o >= 0) if d == 0 else (y + o < SIDE)
                    weight = jnp.exp(rate * (BLOCK * (o - 1.0)))
                    total = total + jnp.where(there, weight * states[source, p].astype(F32), 0.0)
                total = total.astype(BF16)
                zero = jnp.zeros((), BF16)
                carried[p, d * 128:(d + 1) * 128, 0:128] = jnp.where(row_low, total, zero)
                carried[p, d * 128:(d + 1) * 128, 128:256] = jnp.where(row_low, zero, total)

    def finish_rows(r, dst):
        rows = pl.ds(pl.multiple_of(r * ROWS, ROWS), ROWS)
        for p in range(PAIRS):
            outside = matmul(qs[p, rows, :], carried[p])
            for e in range(2):
                h = 2 * p + e
                whole = ret[r, :, h * 128:(h + 1) * 128] + outside[:, e * 128:(e + 1) * 128]
                centred = whole - jnp.mean(whole, axis=-1, keepdims=True)
                var = jnp.mean(centred * centred, axis=-1, keepdims=True)
                dst[:, h * 128:(h + 1) * 128] = (centred * lax.rsqrt(var + EPS)).astype(BF16)

    to_rows = (across, left, right, x)

    def normed(n):
        r = to_rows[n]
        if n == 3:
            finish_rows(r, nb.at[x])
            return
        finish_rows(r, ns.at[n])
        if n == 0:
            send(ns.at[0, h0], relay.at[0], nb_s.at[0], nb_r.at[0], at_x(right))
            send(ns.at[0, h1], relay.at[1], nb_s.at[0], nb_r.at[0], at_x(left))
        else:
            send(ns.at[n], nb.at[x], nb_s.at[0], nb_r.at[1], at_x(r))

    def normed_forward():
        arrive(relay, nb_s.at[0], nb_r.at[0])
        send(relay.at[0], nb.at[left, h0], nb_s.at[0], nb_r.at[1], at_x(right))
        send(relay.at[1], nb.at[right, h1], nb_s.at[0], nb_r.at[1], at_x(left))

    def normed_all():
        arrive(nb.at[pl.ds(0, 3)], nb_s.at[0], nb_r.at[1])

    def output(stage):
        if stage == 0:
            normed_all()
        count = (5, 3)[stage]
        arrive(wo.at[:, pl.ds(0, count)], wod_s.at[0], wod_r.at[stage])
        arrive(wz.at[pl.ds(0, count)], wzd_s.at[0], wzd_r.at[stage])
        offsets = ((0, 1, 7, 2, 6), (3, 5, 4))[stage]
        left_hand, blocks = [], []
        for offset in offsets:
            at = mod(z + offset, RING)
            start = pl.multiple_of(lax.rem(at, 2) * 256, 256)
            left_hand.append(nb[lax.div(at, 2), :, pl.ds(start, 256)])
            blocks.append(pl.ds(at * 2, 2))
        for part in range(SIDE + 1):
            width = PART if part < SIDE else REST
            cols = slice(part * PART, part * PART + width)
            total = jnp.zeros((ROWS, width), F32) if stage == 0 else acc_o[:, cols]
            for lhs, rows in zip(left_hand, blocks):
                weight = wo[part, rows] if part < SIDE else wz[rows]
                total = total + matmul(lhs, weight.reshape(256, width))
            if stage == 0:
                acc_o[:, cols] = total
            else:
                out_ref[0, :, cols] = total.astype(BF16)

    def run(name, task, *arguments):
        with jax.named_scope(name):
            fetched(name)
            task(*arguments)

    run("K0", k_step, 0)
    run("LD", send_rates)
    run("T0", tokens_first)
    run("T1", tokens_second)
    run("O0", o_step, 0)
    run("K1", k_step, 1)
    run("TAB", tables)
    run("Q0", q_step, 0)
    run("LF", forward_rates)
    run("TF", tokens_forward)
    run("O1", o_step, 1)
    run("K2", k_step, 2)
    run("Q1", q_step, 1)
    run("DEC", decays)
    run("O2", o_step, 2)
    run("F1", f_step, 1)
    run("TA", tokens_all)
    run("KA", k_project, 0)
    run("K3", k_step, 3)
    run("QA", q_project, 0)
    run("Q2", q_step, 2)
    run("SO0", own_output_block)
    run("Z0", zz_step, 0)
    run("F2", f_step, 2)
    run("KB", k_project, 1)
    run("D1", d_step, 1)
    run("O3", o_step, 3)
    run("QB", q_project, 1)
    run("G1", g_step, 1)
    run("K4", k_step, 4)
    run("D2", d_step, 2)
    run("G2", g_step, 2)
    run("Q3", q_step, 3)
    run("KC", k_project, 2)
    run("KD", k_project, 3)
    run("RK", keys_values)
    run("Z1", zz_step, 1)
    run("O4", o_step, 4)
    run("F3", f_step, 3)
    run("QC", q_project, 2)
    run("Q4", q_step, 4)
    run("QD", q_project, 3)
    run("RQ", queries)
    run("I0", in_block, to_rows[0])
    run("Z2", zz_step, 2)
    run("I2", in_block, to_rows[2])
    run("CAR", carry_states)
    run("N0", normed, 0)
    run("N2", normed, 2)
    run("I1", in_block, to_rows[1])
    run("N1", normed, 1)
    run("F4", f_step, 4)
    run("I3", in_block, to_rows[3])
    run("D4", d_step, 4)
    run("D3", d_step, 3)
    run("Z3", zz_step, 3)
    run("NF", normed_forward)
    run("G3", g_step, 3)
    run("G4", g_step, 4)
    run("N3", normed, 3)
    run("Z4", zz_step, 4)
    run("OA", output, 0)
    run("OB", output, 1)
    for ref, sem in (
        (tok.at[pl.ds(0, 3)], tok_s), (wq.at[pl.ds(0, 7)], wq_s), (wk.at[pl.ds(0, 7)], wk_s),
        (wz.at[pl.ds(0, 7)], wz_s), (wo.at[0, pl.ds(0, 7)], wo_s), (wq.at[pl.ds(0, 8)], wqd_s),
        (wk.at[pl.ds(0, 8)], wkd_s), (wz.at[pl.ds(0, 8)], wzd_s), (wo.at[:, pl.ds(0, 8)], wod_s),
        (wo.at[0, pl.ds(0, 14)], wy_s), (wo.at[0, pl.ds(0, 7)], wf_s),
        (states.at[pl.ds(0, 3)], st_s), (nb, nb_s),
    ):
        pltpu.make_async_remote_copy(
            src_ref=ref, dst_ref=ref, send_sem=sem.at[0], recv_sem=lr_r.at[0],
            device_id=other_core, device_id_type=pl.DeviceIdType.MESH,
        ).wait_send()
    @pl.when(x != y)
    def _():
        rate_copy().wait_send()

    @pl.when(x == y)
    def _():
        for n, to in enumerate((above, below, facing)):
            rates_copy(n + 1, to).wait_send()


def shards(tokens, query_weight, key_weight, value_weight, output_weight, log_decay):
    half_dim = DK // 2
    frequency = (
        np.float32(10000.0) ** (-np.arange(half_dim, dtype=np.float32) / np.float32(half_dim))
    ).astype(np.float32)
    frequency = jnp.asarray(np.tile(frequency, 4)[None, :])
    anywhere = pl.BlockSpec(memory_space=pl.ANY)
    vmem = pl.BlockSpec(memory_space=pltpu.VMEM)
    dma = pltpu.SemaphoreType.DMA
    return pl.pallas_call(
        kernel,
        out_shape=pltpu.VMEM((1, ROWS, D), BF16),
        in_specs=[anywhere] * 7,
        out_specs=vmem,
        scratch_shapes=[
            pltpu.VMEM((SIDE, ROWS, D), BF16),
            pltpu.VMEM((16, 128, 256), BF16),
            pltpu.VMEM((16, 128, KV), BF16),
            pltpu.VMEM((SIDE, 16, 128, PART), BF16),
            pltpu.VMEM((16, 128, REST), BF16),
            pltpu.VMEM((1, 2), F32),
            pltpu.VMEM((1, 128), F32),
            pltpu.VMEM((8, 128), F32),
            pltpu.VMEM((SIDE, 8, 128), F32),
            pltpu.VMEM((BLOCK, 256), F32),
            pltpu.VMEM((BLOCK, KV), F32),
            pltpu.VMEM((BLOCK, 128), F32),
            pltpu.VMEM((BLOCK, 128), F32),
            pltpu.VMEM((OWN, ROWS, 7 * 128), F32),
            pltpu.VMEM((PAIRS, 4, BLOCK, 128), F32),
            pltpu.VMEM((PAIRS, BLOCK, 128), BF16),
            pltpu.VMEM((PAIRS, BLOCK, 128), BF16),
            pltpu.VMEM((OWN, BLOCK, 128), BF16),
            pltpu.VMEM((PAIRS, BLOCK, 256), BF16),
            pltpu.VMEM((BLOCK, 256), BF16),
            pltpu.VMEM((2, PAIRS, 128, 128), BF16),
            pltpu.VMEM((SIDE, PAIRS, 128, 128), BF16),
            pltpu.VMEM((PAIRS, 256, 256), BF16),
            pltpu.VMEM((SIDE, ROWS, 512), F32),
            pltpu.VMEM((3, ROWS, 512), BF16),
            pltpu.VMEM((2, 64, 512), BF16),
            pltpu.VMEM((SIDE, ROWS, 512), BF16),
            pltpu.VMEM((ROWS, D), F32),
            dma((7,)), dma((1,)), dma((2,)),
            dma((1,)), dma((4,)), dma((1,)), dma((4,)),
            dma((1,)), dma((4,)), dma((1,)), dma((4,)),
            dma((1,)), dma((4,)),
            dma((1,)), dma((4,)), dma((1,)), dma((4,)),
            dma((1,)), dma((2,)),
            dma((1,)), dma((4,)), dma((1,)), dma((2,)),
            dma((1,)), dma((1,)), dma((1,)), dma((2,)), dma((4,)), dma((1,)), dma((1,)),
        ],
        compiler_params=pltpu.CompilerParams(
            collective_id=0, has_side_effects=True, vmem_limit_bytes=60 * 1024 * 1024
        ),
        name="retention",
    )(
        tokens, query_weight, key_weight, value_weight, output_weight, log_decay.T, frequency
    )


def solution(mesh):
    placed = (
        P("dp", "sp", None),
        P("dp", None),
        P("dp", None),
        P("dp", None),
        P("dp", None),
        P(None, "sp"),
    )
    return jax.shard_map(
        shards, mesh=mesh, in_specs=placed, out_specs=P("dp", "sp", None), check_vma=False
    )
```
